32 devices in a mesh: sp: 8 (over z, x), tp: 4 (over y, core).
Axes of the slice: x: 2, y: 2, z: 4, core: 2. Of those that a mesh axis runs over, the one named last changes fastest.
Arguments:
- tokens: bfloat16 [3072, 2048], P(('sp', 'tp')), may hold values from -6 to 6
- norm_gain: float32 [2048], replicated, may hold values from 0.1 to 1.9
- w_recept: bfloat16 [2048, 1024], P(None, 'tp'), may hold values from -0.125 to 0.125
- w_key: bfloat16 [2048, 1024], P(None, 'tp'), may hold values from -0.125 to 0.125
- w_value: bfloat16 [2048, 1024], P(None, 'tp'), may hold values from -0.125 to 0.125
- w_decay: bfloat16 [2048, 1024], P(None, 'tp'), may hold values from -0.125 to 0.125
- w_rate: bfloat16 [2048, 1024], P(None, 'tp'), may hold values from -0.125 to 0.125
- w_gate: bfloat16 [2048, 1024], P(None, 'tp'), may hold values from -0.125 to 0.125
- shift_mix: float32 [3, 1024], P(None, 'tp'), may hold values from 0 to 1
- decay_base: float32 [1024], P('tp'), may hold values from -16 to -2
- rate_base: float32 [1024], P('tp'), may hold values from -10 to 1
- decay_drift: float32 [3072], P('sp'), may hold values from -2 to 2, as said below
- group_gain: float32 [1024], P('tp'), may hold values from 0.1 to 1.9
- initial_state: float32 [16, 64, 64], P('tp'), may hold values from -240 to 240
- w_out: bfloat16 [1024, 2048], replicated, may hold values from -0.1875 to 0.1875
Outputs:
- out: bfloat16 [3072, 2048], P(('sp', 'tp'))
The draws below stay inside these ranges and needn't reach their ends.
Inputs may be any that keep to these rules, and one draw needn't show every extreme that they name: `decay_drift`: constant over aligned runs of 64 positions.
All inputs are finite; a program needn't handle non-finite values.
Results may differ from the reference program's by a relative error of at most 0.0083.
Values may be sent and summed in bfloat16 or wider, within the bound.
A program may use at most 128 MiB of HBM per device.

```python
import math
import jax
import jax.numpy as jnp
from jax import lax

D = 2048
HEADS = 16
HEAD = 64
BLOCK = 64
INNER = 1024
TOKENS = 3072


def head_kinds(key):
    picks = jax.random.randint(jax.random.fold_in(key, 11), (HEADS,), 0, 8)
    return picks < 4


def draw_decay_base(key, part):
    slow = head_kinds(key)
    jitter = jax.random.uniform(jax.random.fold_in(key, 12), (HEADS, HEAD), jnp.float32, -0.5, 0.5)
    long_level = -math.log(TOKENS) - 1.0
    value = jnp.where(slow[:, None], long_level, -3.0) + jitter
    return value.reshape(HEADS * HEAD).astype(jnp.float32)


def draw_rate_base(key, part):
    slow = head_kinds(key)
    jitter = jax.random.uniform(jax.random.fold_in(key, 13), (HEADS, HEAD), jnp.float32, -1.0, 1.0)
    long_level = math.log(HEAD / TOKENS) - 1.0
    value = jnp.where(slow[:, None], long_level + 0.5 * jitter, jitter)
    return value.reshape(HEADS * HEAD).astype(jnp.float32)


def draw_decay_drift(key, part):
    count = TOKENS // BLOCK
    levels = jax.random.uniform(jax.random.fold_in(key, 14), (count,), jnp.float32, -1.5, 1.5)
    return jnp.repeat(levels, BLOCK).astype(jnp.float32)


def level_of(own_key, dims, cuts, low, high):
    gain, own = 1.0, jax.random.fold_in(own_key, 6)
    for position, shards_of in cuts:
        draws = jnp.exp(jax.random.uniform(jax.random.fold_in(own, position), (shards_of,), jnp.float32, low / len(cuts), high / len(cuts)))
        gain = gain * jnp.repeat(draws, dims[position] // shards_of).reshape([-1 if axis == position else 1 for axis in range(len(dims))])
    return gain


def gaussian(rng, extent, width, limit, cuts=(), held_as=jnp.bfloat16):
    drawn = jax.random.normal(rng, extent, jnp.float32) * width
    if len(cuts) > 0:
        drawn = level_of(rng, extent, cuts, -0.22, 0.18) * drawn
    return jnp.clip(drawn, min=-limit, max=limit).astype(held_as)


def setup_inputs(seed: int = 0) -> dict:
    arg_keys = jax.random.split(jax.random.key(seed), 16)
    return {
        "tokens": gaussian(arg_keys[0], (TOKENS, D), 1.0, 6.0, ((0, 32),)),
        "norm_gain": jnp.clip(1.0 + 0.18 * jax.random.normal(arg_keys[1], (D,), jnp.float32), 0.1, 1.9),
        "w_recept": gaussian(arg_keys[2], (D, INNER), D ** -0.5, 0.125, ((1, 4),)),
        "w_key": gaussian(arg_keys[3], (D, INNER), D ** -0.5, 0.125, ((1, 4),)),
        "w_value": gaussian(arg_keys[4], (D, INNER), D ** -0.5, 0.125, ((1, 4),)),
        "w_decay": gaussian(arg_keys[5], (D, INNER), D ** -0.5, 0.125, ((1, 4),)),
        "w_rate": gaussian(arg_keys[6], (D, INNER), D ** -0.5, 0.125, ((1, 4),)),
        "w_gate": gaussian(arg_keys[7], (D, INNER), D ** -0.5, 0.125, ((1, 4),)),
        "shift_mix": jnp.clip(1.0 * jax.random.uniform(arg_keys[8], (3, INNER), jnp.float32) ** level_of(arg_keys[8], (3, INNER), ((1, 4),), -0.2, 0.2), 0.0, 1.0),
        "decay_base": draw_decay_base(jax.random.fold_in(arg_keys[15], 71), 0),
        "rate_base": draw_rate_base(jax.random.fold_in(arg_keys[15], 71), 0),
        "decay_drift": draw_decay_drift(jax.random.fold_in(arg_keys[15], 71), 0),
        "group_gain": jnp.clip(1.0 + 0.18 * jax.random.normal(arg_keys[12], (INNER,), jnp.float32), 0.1, 1.9),
        "initial_state": gaussian(arg_keys[13], (HEADS, HEAD, HEAD), 40.0, 240.0, ((0, 4),), jnp.float32),
        "w_out": gaussian(arg_keys[14], (INNER, D), INNER ** -0.5, 0.1875),
    }


norm_floor = 0.5
group_floor = 1.0
highest = lax.Precision.HIGHEST

def reference(tokens, norm_gain, w_recept, w_key, w_value, w_decay, w_rate, w_gate, shift_mix, decay_base, rate_base, decay_drift, group_gain, initial_state, w_out):
    tok_float = tokens.astype(jnp.float32)
    normed = (tok_float * lax.rsqrt(lax.optimization_barrier(jnp.mean(tok_float * tok_float, axis=-1, keepdims=True)) + norm_floor) * norm_gain).astype(jnp.bfloat16)

    def project(weight):
        return jnp.dot(normed, weight, preferred_element_type=jnp.float32).astype(jnp.bfloat16)

    def shifted(raw_proj, mix_row):
        current = raw_proj.astype(jnp.float32)
        earlier = jnp.concatenate([jnp.zeros((1, current.shape[1]), jnp.float32), current[:-1]], axis=0)
        return current + (earlier - current) * mix_row
    recept = shifted(project(w_recept), shift_mix[0])
    key = shifted(project(w_key), shift_mix[1])
    value = shifted(project(w_value), shift_mix[2])
    level = decay_base + project(w_decay).astype(jnp.float32) + decay_drift[:, None]
    decay = jnp.exp(-jnp.exp(-jax.nn.softplus(-level) - 0.5))
    rate = jax.nn.sigmoid(rate_base + project(w_rate).astype(jnp.float32))
    gate = jax.nn.sigmoid(project(w_gate).astype(jnp.float32))

    def heads(array):
        return array.reshape(TOKENS, HEADS, HEAD)
    key_heads = heads(key)
    unit = key_heads * lax.rsqrt(lax.optimization_barrier(jnp.sum(key_heads * key_heads, axis=-1, keepdims=True)) + 1.0)

    def advance(state, inputs):
        recept_now, decay_now, key_now, value_now, unit_now, rate_now = inputs
        removed = jnp.einsum('hvk,hk->hv', state, unit_now, precision=highest)
        state = state * decay_now[:, None, :] - removed[:, :, None] * (unit_now * rate_now)[:, None, :] + value_now[:, :, None] * key_now[:, None, :]
        return (state, jnp.einsum('hvk,hk->hv', state, recept_now, precision=highest))
    _, mixed = lax.scan(advance, initial_state, (heads(recept), heads(decay), key_heads, heads(value), unit, heads(rate)))
    center = mixed - lax.optimization_barrier(jnp.mean(mixed, axis=-1, keepdims=True))
    spread = lax.optimization_barrier(jnp.mean(center * center, axis=-1, keepdims=True))
    scaled = center * lax.rsqrt(spread + group_floor) * group_gain.reshape(HEADS, HEAD)
    gated = (scaled.reshape(TOKENS, INNER) * gate).astype(jnp.bfloat16)
    return jnp.dot(gated, w_out, preferred_element_type=jnp.float32).astype(jnp.bfloat16)
```

```python
import functools

import jax
import jax.numpy as jnp
from jax import lax
from jax.experimental import pallas as pl
from jax.experimental.pallas import tpu as pltpu
from jax.sharding import PartitionSpec as P

HEAD = 64
BLOCK = 64
F32 = jnp.float32
BF16 = jnp.bfloat16

norm_floor = 0.5
group_floor = 1.0

NN = (((1,), (0,)), ((), ()))
NT = (((1,), (1,)), ((), ()))
TN = (((0,), (0,)), ((), ()))


def dot1(a, b, dims):
    return lax.dot_general(a, b, dims, preferred_element_type=F32)


def split(a):
    high = a.astype(BF16)
    return high, (a - high.astype(F32)).astype(BF16)


def mm(a, b, dims=NN):
    ah, al = split(a)
    bh, bl = split(b)
    return dot1(ah, bh, dims) + (dot1(ah, bl, dims) + dot1(al, bh, dims))


def sum_rows(a, ones):
    high, rest = split(a)
    mid, low = split(a - high.astype(F32))
    return dot1(ones, high, NN) + (dot1(ones, mid, NN) + dot1(ones, low, NN))


def scan_kernel(
    n,
    m,
    heads,
    blocks,
    drift_ref,
    proj_ref,
    edge_ref,
    mix_ref,
    dbase_ref,
    rbase_ref,
    gain_ref,
    init_ref,
    wout_ref,
    out_ref,
    last_row,
    reads,
    prefix,
    running,
    window,
    g_buf,
    r_buf,
    flat,
    gated,
    act,
    wout,
    w_sem,
    g_send,
    g_recv,
    a_send,
    a_recv,
):
    s = lax.axis_index("sp")
    t = lax.axis_index("tp")
    steps = []
    while (1 << len(steps)) < n:
        steps.append(1 << len(steps))

    barrier = pltpu.get_barrier_semaphore()
    for d in steps:
        for other, ok in ((s + d, s + d < n), (s - d, s - d >= 0)):

            @pl.when(ok)
            def _():
                pl.semaphore_signal(
                    barrier, inc=1, device_id={"sp": other, "tp": t}, device_id_type=pl.DeviceIdType.MESH
                )

    for q in range(1, m):
        pl.semaphore_signal(
            barrier, inc=1, device_id={"sp": s, "tp": lax.rem(t + q, m)}, device_id_type=pl.DeviceIdType.MESH
        )

    load = pltpu.make_async_copy(wout_ref, wout, w_sem)
    load.start()

    width = BLOCK
    rows_i = lax.broadcasted_iota(jnp.int32, (width, width), 0)
    cols_i = lax.broadcasted_iota(jnp.int32, (width, width), 1)
    strict = cols_i < rows_i
    incl = cols_i <= rows_i
    eye = jnp.where(cols_i == rows_i, 1.0, 0.0).astype(F32)
    ones = jnp.where(incl, 1.0, 0.0).astype(BF16)
    zeros = jnp.zeros((width, HEAD), F32)
    levels = []
    size = 1
    while size < width:
        same = (rows_i // (2 * size)) == (cols_i // (2 * size))
        levels.append(same & ((rows_i // size) % 2 == 1) & ((cols_i // size) % 2 == 0))
        size *= 2
    first_row = lax.broadcasted_iota(jnp.int32, (width, heads * HEAD), 0) == 0
    mix = mix_ref[...]
    dbase = dbase_ref[...].reshape(1, heads * HEAD)
    rbase = rbase_ref[...].reshape(1, heads * HEAD)
    gain = gain_ref[...].reshape(1, heads * HEAD)

    for j in range(3):
        last_row[j] = jnp.broadcast_to(edge_ref[j].astype(F32), (8, heads * HEAD))
    for h in range(heads):
        running[h] = jnp.concatenate([eye, zeros], axis=1)

    @pl.loop(0, blocks)
    def _(b):
        at = pl.ds(pl.multiple_of(b * width, width), width)

        def shifted(j):
            cur = proj_ref[j, at, :].astype(F32)
            earlier = jnp.where(first_row, last_row[j, 0:1, :], pltpu.roll(cur, 1, 0))
            last_row[j] = jnp.broadcast_to(cur[width - 1 :, :], (8, heads * HEAD))
            return cur + (earlier - cur) * mix[j : j + 1, :]

        recept, key, value = shifted(0), shifted(1), shifted(2)
        level = dbase + proj_ref[3, at, :].astype(F32) + drift_ref[b * width]
        logs = -0.6065306597126334 * jax.nn.sigmoid(level)
        rate = jax.nn.sigmoid(rbase + proj_ref[4, at, :].astype(F32))
        total = sum_rows(logs, ones)
        through = jnp.exp(total)
        until = jnp.exp(total - logs)
        inverse = jnp.exp(-total)
        key_s = key * inverse
        rec_s = recept * through
        final = through[width - 1 :, :]
        rate_inv = rate * inverse
        for h in range(heads):
            ch = slice(h * HEAD, (h + 1) * HEAD)
            key_h = key[:, ch]
            unit = key_h * lax.rsqrt(jnp.sum(key_h * key_h, axis=1, keepdims=True) + 1.0)
            val_h = value[:, ch]
            alpha = -unit * until[:, ch]
            beta = unit * rate_inv[:, ch]
            key_sh = key_s[:, ch]
            rec_h = rec_s[:, ch]
            fin = final[:, ch]
            cross = mm(
                jnp.concatenate([alpha, rec_h], axis=0), jnp.concatenate([beta, key_sh], axis=0), NT
            )
            low_ab = jnp.where(strict, cross[:width, :width], 0.0)
            low_ak = jnp.where(strict, cross[:width, width:], 0.0)
            up_b = jnp.where(incl, cross[width:, :width], 0.0)
            up_k = jnp.where(incl, cross[width:, width:], 0.0)
            both = mm(jnp.concatenate([low_ak, up_k], axis=0), val_h)
            inv = eye + jnp.where(levels[0], low_ab, 0.0)
            for mask in levels[1:]:
                inv = inv + mm(inv, mm(jnp.where(mask, low_ab, 0.0), inv))
            solved = mm(inv, jnp.concatenate([alpha, both[:width]], axis=1))
            reads[b, h] = jnp.concatenate([rec_h, both[width:]], axis=1) + mm(up_b, solved)
            ends = jnp.concatenate([beta * fin, key_sh * fin], axis=0)
            piece = mm(
                ends, jnp.concatenate([solved, jnp.concatenate([zeros, val_h], axis=1)], axis=0), TN
            )
            trans = piece[:, :HEAD] + eye * fin
            before = running[h]
            prefix[b, h] = before
            running[h] = mm(trans, before) + jnp.concatenate([zeros, piece[:, HEAD:]], axis=1)

    count = m - 1
    for d in steps:
        count = count + (s + d < n).astype(jnp.int32) + (s - d >= 0).astype(jnp.int32)
    pl.semaphore_wait(barrier, count)

    def joined(later, earlier):
        return mm(later[:, :HEAD], earlier) + jnp.concatenate([zeros, later[:, HEAD:]], axis=1)

    at_start = s == 0
    for h in range(heads):
        own = running[h]
        start = jnp.concatenate([zeros, init_ref[h].T], axis=1)
        window[h] = jnp.where(at_start, start, jnp.concatenate([eye, zeros], axis=1))
        g_buf[0, h] = jnp.where(at_start, joined(own, start), own)

    def hop(k):
        return pltpu.make_async_remote_copy(
            src_ref=g_buf.at[k],
            dst_ref=r_buf.at[k],
            send_sem=g_send.at[k],
            recv_sem=g_recv.at[k],
            device_id={"sp": s + steps[k], "tp": t},
            device_id_type=pl.DeviceIdType.MESH,
        )

    for k, d in enumerate(steps):

        @pl.when(s + d < n)
        def _():
            hop(k).start()

        @pl.when(s - d >= 0)
        def _():
            hop(k).wait_recv()
            for h in range(heads):
                window[h] = joined(window[h], r_buf[k, h])

        if k + 1 < len(steps):
            for h in range(heads):
                g_buf[k + 1, h] = jnp.where(at_start, g_buf[k, h], joined(running[h], window[h]))

    @pl.loop(0, blocks)
    def _(b):
        at = pl.ds(pl.multiple_of(b * width, width), width)
        gate = jax.nn.sigmoid(proj_ref[5, at, :].astype(F32))
        pieces = []
        for h in range(heads):
            ch = slice(h * HEAD, (h + 1) * HEAD)
            now = prefix[b, h]
            state = mm(now[:, :HEAD], window[h][:, HEAD:]) + now[:, HEAD:]
            read = reads[b, h]
            mixed = mm(read[:, :HEAD], state) + read[:, HEAD:]
            center = mixed - jnp.mean(mixed, axis=1, keepdims=True)
            spread = jnp.mean(center * center, axis=1, keepdims=True)
            pieces.append(center * lax.rsqrt(spread + group_floor))
        gated[at, :] = (jnp.concatenate(pieces, axis=1) * gain * gate).astype(BF16)

    share = act.shape[1]

    def part(q):
        dest = lax.rem(t + q, m)
        return pltpu.make_async_remote_copy(
            src_ref=gated.at[pl.ds(pl.multiple_of(dest * share, share), share), :],
            dst_ref=act.at[t],
            send_sem=a_send.at[q],
            recv_sem=a_recv.at[q],
            device_id={"sp": s, "tp": dest},
            device_id_type=pl.DeviceIdType.MESH,
        )

    for q in range(1, m):
        part(q).start()
    act[t] = gated[pl.ds(pl.multiple_of(t * share, share), share), :]
    load.wait()
    for q in range(1, m):
        part(q).wait_recv()
    rows = jnp.concatenate([act[q] for q in range(m)], axis=1)
    columns = out_ref.shape[1]
    tile = min(512, columns)
    for c in range(0, columns, tile):
        out_ref[:, c : c + tile] = dot1(rows, wout[:, c : c + tile], NN).astype(BF16)
    for q in range(1, m):
        part(q).wait_send()
    for k, d in enumerate(steps):

        @pl.when(s + d < n)
        def _():
            hop(k).wait_send()


def scan_call(n, m, drift, proj, edge, mix, dbase, rbase, gain, init, w_out):
    seq, width = proj.shape[1:]
    heads, blocks = width // HEAD, seq // BLOCK
    hops = max(1, (n - 1).bit_length())
    vmem = pl.BlockSpec(memory_space=pltpu.VMEM)
    return pl.pallas_call(
        functools.partial(scan_kernel, n, m, heads, blocks),
        out_shape=jax.ShapeDtypeStruct((seq // m, w_out.shape[1]), BF16),
        in_specs=[pl.BlockSpec(memory_space=pltpu.SMEM)]
        + [vmem] * 7
        + [pl.BlockSpec(memory_space=pl.ANY)],
        out_specs=vmem,
        scratch_shapes=[
            pltpu.VMEM((3, 8, width), F32),
            pltpu.VMEM((blocks, heads, BLOCK, 2 * HEAD), F32),
            pltpu.VMEM((blocks, heads, HEAD, 2 * HEAD), F32),
            pltpu.VMEM((heads, HEAD, 2 * HEAD), F32),
            pltpu.VMEM((heads, HEAD, 2 * HEAD), F32),
            pltpu.VMEM((hops, heads, HEAD, 2 * HEAD), F32),
            pltpu.VMEM((hops, heads, HEAD, 2 * HEAD), F32),
            pltpu.VMEM((8, 128), F32),
            pltpu.VMEM((seq, width), BF16),
            pltpu.VMEM((m, seq // m, width), BF16),
            pltpu.VMEM(w_out.shape, BF16),
            pltpu.SemaphoreType.DMA,
            pltpu.SemaphoreType.DMA((hops,)),
            pltpu.SemaphoreType.DMA((hops,)),
            pltpu.SemaphoreType.DMA((m,)),
            pltpu.SemaphoreType.DMA((m,)),
        ],
        compiler_params=pltpu.CompilerParams(
            collective_id=1, has_side_effects=True, vmem_limit_bytes=48 * 1024 * 1024
        ),
        name="scan_kernel",
    )(drift, proj, edge, mix, dbase, rbase, gain, init, w_out)


def shifted_2(block, axis, distance):
    devices = range(lax.axis_size(axis))
    route = [(i - distance, i) for i in devices if i - distance in devices]
    return lax.ppermute(block, axis, route)


def per_device(
    n,
    m,
    tokens,
    norm_gain,
    w_recept,
    w_key,
    w_value,
    w_decay,
    w_rate,
    w_gate,
    shift_mix,
    decay_base,
    rate_base,
    decay_drift,
    group_gain,
    initial_state,
    w_out,
):
    tok_float = tokens.astype(F32)
    normed = (
        tok_float
        * lax.rsqrt(jnp.mean(tok_float * tok_float, axis=-1, keepdims=True) + norm_floor)
        * norm_gain
    ).astype(BF16)
    weights = (w_recept, w_key, w_value, w_decay, w_rate, w_gate)
    piece = lax.all_gather(normed, "tp", axis=0, tiled=True)
    projected = jnp.stack(
        [jnp.dot(piece, weight, preferred_element_type=F32).astype(BF16) for weight in weights], axis=0
    )
    edge = shifted_2(projected[0:3, -1:, :], "sp", 1)
    return scan_call(
        n, m, decay_drift, projected, edge, shift_mix, decay_base, rate_base, group_gain, initial_state, w_out
    )


def solution(mesh):
    return jax.shard_map(
        functools.partial(per_device, mesh.shape["sp"], mesh.shape["tp"]),
        mesh=mesh,
        in_specs=(
            P(("sp", "tp"), None),
            P(),
            P(None, "tp"),
            P(None, "tp"),
            P(None, "tp"),
            P(None, "tp"),
            P(None, "tp"),
            P(None, "tp"),
            P(None, "tp"),
            P("tp"),
            P("tp"),
            P("sp"),
            P("tp"),
            P("tp", None, None),
            P(),
        ),
        out_specs=P(("sp", "tp"), None),
        check_vma=False,
    )
```

```python
import functools

import jax
import jax.numpy as jnp
from jax import lax
from jax.experimental import pallas as pl
from jax.experimental.pallas import tpu as pltpu
from jax.sharding import PartitionSpec as P

HEAD = 64
BLOCK = 64
F32 = jnp.float32
BF16 = jnp.bfloat16

norm_floor = 0.5
group_floor = 1.0

NN = (((1,), (0,)), ((), ()))
NT = (((1,), (1,)), ((), ()))
TN = (((0,), (0,)), ((), ()))


def dot1(a, b, dims):
    return lax.dot_general(a, b, dims, preferred_element_type=F32)


def split(a):
    high = a.astype(BF16)
    return high, (a - high.astype(F32)).astype(BF16)


def mm(a, b, dims=NN):
    ah, al = split(a)
    bh, bl = split(b)
    return dot1(ah, bh, dims) + (dot1(ah, bl, dims) + dot1(al, bh, dims))


def sum_rows(a, ones):
    high, rest = split(a)
    mid, low = split(a - high.astype(F32))
    return dot1(ones, high, NN) + (dot1(ones, mid, NN) + dot1(ones, low, NN))


def layer_kernel(
    n,
    m,
    heads,
    blocks,
    drift_ref,
    tok_ref,
    ngain_ref,
    wr_ref,
    wk_ref,
    wv_ref,
    wd_ref,
    wa_ref,
    wg_ref,
    mix_ref,
    dbase_ref,
    rbase_ref,
    gain_ref,
    init_ref,
    wout_ref,
    out_ref,
    tok,
    edge_out,
    edge_in,
    normed,
    weights,
    proj,
    edges,
    last_row,
    reads,
    pieces,
    prefix,
    running,
    window,
    g_buf,
    r_buf,
    gated,
    act,
    wout,
    own_sem,
    w_sem,
    t_send,
    t_recv,
    f_send,
    f_recv,
    e_send,
    e_recv,
    g_send,
    g_recv,
    a_send,
    a_recv,
):
    s = lax.axis_index("sp")
    t = lax.axis_index("tp")
    half = m // 2
    upper = t // half
    base = upper * half
    across = lax.rem(t + half, m)
    share, depth = tok_ref.shape
    lanes = edge_out.shape[1]
    width = BLOCK
    channels = heads * HEAD
    steps = []
    while (1 << len(steps)) < n:
        steps.append(1 << len(steps))

    def near(q):
        return base + lax.rem(t - base + q, half)

    own_load = pltpu.make_async_copy(tok_ref, tok.at[t], own_sem)
    own_load.start()
    sources = (wr_ref, wk_ref, wv_ref, wd_ref, wa_ref, wg_ref)
    loads = [
        pltpu.make_async_copy(ref, weights.at[j], w_sem.at[j]) for j, ref in enumerate(sources)
    ]
    for load in loads:
        load.start()
    out_load = pltpu.make_async_copy(wout_ref, wout, w_sem.at[len(sources)])
    out_load.start()

    barrier = pltpu.get_barrier_semaphore()
    count = m - 1

    def greet(sp, tp):
        pl.semaphore_signal(
            barrier, inc=1, device_id={"sp": sp, "tp": tp}, device_id_type=pl.DeviceIdType.MESH
        )

    for q in range(1, m):
        greet(s, lax.rem(t + q, m))
    for d in steps:
        for other, ok in ((s + d, s + d < n), (s - d, s - d >= 0)):
            count = count + ok.astype(jnp.int32)

            @pl.when(ok)
            def _():
                greet(other, t)

    for q in range(m - 1):
        sends = jnp.logical_and(t == m - 1, s + 1 < n)
        takes = jnp.logical_and(t == q, s >= 1)
        count = count + sends.astype(jnp.int32) + takes.astype(jnp.int32)

        @pl.when(sends)
        def _():
            greet(s + 1, q)

        @pl.when(takes)
        def _():
            greet(s - 1, m - 1)

    own_load.wait()
    last = tok[t, share - 16 :, :].astype(F32)[15:16, :]
    for i in range(depth // lanes):
        edge_out[i : i + 1, :] = last[:, i * lanes : (i + 1) * lanes]
    pl.semaphore_wait(barrier, count)

    def remote(src, dst, send, recv, sp, tp):
        return pltpu.make_async_remote_copy(
            src_ref=src,
            dst_ref=dst,
            send_sem=send,
            recv_sem=recv,
            device_id={"sp": sp, "tp": tp},
            device_id_type=pl.DeviceIdType.MESH,
        )

    def token_copy(q):
        other = across if q == 0 else near(q)
        return remote(tok.at[t], tok.at[t], t_send.at[q], t_recv.at[q], s, other)

    def forward_copy(q):
        return remote(tok.at[across], tok.at[across], f_send.at[q], f_recv.at[q], s, near(q))

    def edge_copy(q):
        return remote(edge_out, edge_in.at[0], e_send.at[q], e_recv.at[0], s + 1, q)

    def middle_copy(q):
        return remote(edge_out, edge_in.at[1], e_send.at[q], e_recv.at[1], s, half + q)

    has_next = jnp.logical_and(t == m - 1, s + 1 < n)
    has_middle = t == half - 1

    @pl.when(has_next)
    def _():
        for q in range(m):
            edge_copy(q).start()

    @pl.when(has_middle)
    def _():
        for q in range(half):
            middle_copy(q).start()

    for q in range(half):
        token_copy(q).start()

    rows_i = lax.broadcasted_iota(jnp.int32, (width, width), 0)
    cols_i = lax.broadcasted_iota(jnp.int32, (width, width), 1)
    strict = cols_i < rows_i
    incl = cols_i <= rows_i
    eye = jnp.where(cols_i == rows_i, 1.0, 0.0).astype(F32)
    ones = jnp.where(incl, 1.0, 0.0).astype(BF16)
    zeros = jnp.zeros((width, HEAD), F32)
    levels = []
    size = 1
    while size < width:
        same = (rows_i // (2 * size)) == (cols_i // (2 * size))
        levels.append(same & ((rows_i // size) % 2 == 1) & ((cols_i // size) % 2 == 0))
        size *= 2
    first_row = lax.broadcasted_iota(jnp.int32, (width, channels), 0) == 0
    mix = mix_ref[...]
    dbase = dbase_ref[...].reshape(1, channels)
    rbase = rbase_ref[...].reshape(1, channels)
    gain = gain_ref[...].reshape(1, channels)
    ngain = ngain_ref[...].reshape(1, depth)

    def norm(x):
        scale = lax.rsqrt(jnp.mean(x * x, axis=1, keepdims=True) + norm_floor)
        return (x * scale * ngain).astype(BF16)

    tile = 32
    span = half * share

    def norm_block(owner, place):
        @pl.loop(0, share // tile)
        def _(i):
            rows = pl.ds(pl.multiple_of(i * tile, tile), tile)
            to = pl.ds(pl.multiple_of(place * share + i * tile, tile), tile)
            normed[to, :] = norm(tok[owner, rows, :].astype(F32))

    def project(first, extra):
        to = pl.ds(pl.multiple_of(first * share, share), span)
        for j in range(len(sources)):
            if extra:
                loads[j].wait()
            if extra and j < 3:
                made = dot1(normed[...], weights[j], NN).astype(BF16)
                edges[j] = made[span:, :].astype(F32)
                proj[j, to, :] = made[:span, :]
            else:
                proj[j, to, :] = dot1(normed[:span, :], weights[j], NN).astype(BF16)

    def prepare(b):
        at = pl.ds(pl.multiple_of(b * width, width), width)

        def shifted(j):
            cur = proj[j, at, :].astype(F32)
            earlier = jnp.where(first_row, last_row[j, 0:1, :], pltpu.roll(cur, 1, 0))
            last_row[j] = jnp.broadcast_to(cur[width - 1 :, :], (8, channels))
            return cur + (earlier - cur) * mix[j : j + 1, :]

        recept, key, value = shifted(0), shifted(1), shifted(2)
        level = dbase + proj[3, at, :].astype(F32) + drift_ref[b * width]
        logs = -0.6065306597126334 * jax.nn.sigmoid(level)
        rate = jax.nn.sigmoid(rbase + proj[4, at, :].astype(F32))
        total = sum_rows(logs, ones)
        through = jnp.exp(total)
        until = jnp.exp(total - logs)
        inverse = jnp.exp(-total)
        key_s = key * inverse
        rec_s = recept * through
        final = through[width - 1 :, :]
        rate_inv = rate * inverse
        every = range(heads)
        chans = [slice(h * HEAD, (h + 1) * HEAD) for h in every]
        units = []
        for ch in chans:
            key_h = key[:, ch]
            units.append(key_h * lax.rsqrt(jnp.sum(key_h * key_h, axis=1, keepdims=True) + 1.0))
        alphas = [-units[h] * until[:, chans[h]] for h in every]
        betas = [units[h] * rate_inv[:, chans[h]] for h in every]
        keys = [key_s[:, ch] for ch in chans]
        recs = [rec_s[:, ch] for ch in chans]
        vals = [value[:, ch] for ch in chans]
        fins = [final[:, ch] for ch in chans]
        cross = [
            mm(
                jnp.concatenate([alphas[h], recs[h]], axis=0),
                jnp.concatenate([betas[h], keys[h]], axis=0),
                NT,
            )
            for h in every
        ]
        low_ab = [jnp.where(strict, c[:width, :width], 0.0) for c in cross]
        low_ak = [jnp.where(strict, c[:width, width:], 0.0) for c in cross]
        up_b = [jnp.where(incl, c[width:, :width], 0.0) for c in cross]
        up_k = [jnp.where(incl, c[width:, width:], 0.0) for c in cross]
        both = [mm(jnp.concatenate([low_ak[h], up_k[h]], axis=0), vals[h]) for h in every]
        inv = [eye + jnp.where(levels[0], low, 0.0) for low in low_ab]
        for mask in levels[1:]:
            right = [mm(jnp.where(mask, low_ab[h], 0.0), inv[h]) for h in every]
            inv = [inv[h] + mm(inv[h], right[h]) for h in every]
        solved = [
            mm(inv[h], jnp.concatenate([alphas[h], both[h][:width]], axis=1)) for h in every
        ]
        for h in every:
            reads[b, h] = jnp.concatenate([recs[h], both[h][width:]], axis=1) + mm(
                up_b[h], solved[h]
            )
        for h in every:
            ends = jnp.concatenate([betas[h] * fins[h], keys[h] * fins[h]], axis=0)
            piece = mm(
                ends,
                jnp.concatenate(
                    [solved[h], jnp.concatenate([zeros, vals[h]], axis=1)], axis=0
                ),
                TN,
            )
            pieces[b, h] = piece + jnp.concatenate([eye * fins[h], zeros], axis=1)

    def open_half(which):
        for j in range(3):
            row = jnp.where(which == 0, edges[j, 0:1, :], edges[j, 1:2, :])
            last_row[j] = jnp.broadcast_to(row, (8, channels))

    norm_block(t, t - base)
    for q in range(1, half):
        token_copy(q).wait_recv()
        norm_block(near(half - q), near(half - q) - base)

    @pl.when(s >= 1)
    def _():
        remote(edge_out, edge_in.at[0], e_send.at[0], e_recv.at[0], s, t).wait_recv()

    @pl.when(s == 0)
    def _():
        edge_in[0] = jnp.zeros(edge_in.shape[1:], F32)

    @pl.when(upper == 1)
    def _():
        remote(edge_out, edge_in.at[1], e_send.at[0], e_recv.at[1], s, t).wait_recv()

    @pl.when(upper == 0)
    def _():
        row = tok[half - 1, share - 16 :, :].astype(F32)[15:16, :]
        for i in range(depth // lanes):
            edge_in[1, i : i + 1, :] = row[:, i * lanes : (i + 1) * lanes]

    joined_rows = [
        jnp.concatenate([edge_in[k, i : i + 1, :] for i in range(depth // lanes)], axis=1)
        for k in range(2)
    ]
    normed[span:, :] = norm(
        jnp.concatenate(joined_rows + [jnp.zeros((14, depth), F32)], axis=0)
    )
    project(base, True)
    open_half(upper)

    @pl.loop(0, blocks // 2)
    def _(i):
        prepare(upper * (blocks // 2) + i)

        @pl.when(i == 0)
        def _():
            token_copy(0).wait_recv()
            for q in range(1, half):
                forward_copy(q).start()

    lower = 1 - upper
    norm_block(across, across - lower * half)
    for q in range(1, half):
        forward_copy(q).wait_recv()
        far = lower * half + near(half - q) - base
        norm_block(far, far - lower * half)
    project(lower * half, False)
    open_half(lower)

    @pl.loop(0, blocks // 2)
    def _(i):
        prepare(lower * (blocks // 2) + i)

    def joined(later, earlier):
        return mm(later[:, :HEAD], earlier) + jnp.concatenate([zeros, later[:, HEAD:]], axis=1)

    for h in range(heads):
        running[h] = jnp.concatenate([eye, zeros], axis=1)

    @pl.loop(0, blocks)
    def _(b):
        for h in range(heads):
            prefix[b, h] = running[h]
            running[h] = joined(pieces[b, h], running[h])

    at_start = s == 0
    for h in range(heads):
        own = running[h]
        start = jnp.concatenate([zeros, init_ref[h].T], axis=1)
        window[h] = jnp.where(at_start, start, jnp.concatenate([eye, zeros], axis=1))
        g_buf[0, h] = jnp.where(at_start, joined(own, start), own)

    def hop(k):
        return remote(g_buf.at[k], r_buf.at[k], g_send.at[k], g_recv.at[k], s + steps[k], t)

    for k, d in enumerate(steps):

        @pl.when(s + d < n)
        def _():
            hop(k).start()

        @pl.when(s - d >= 0)
        def _():
            hop(k).wait_recv()
            for h in range(heads):
                window[h] = joined(window[h], r_buf[k, h])

        if k + 1 < len(steps):
            for h in range(heads):
                g_buf[k + 1, h] = jnp.where(at_start, g_buf[k, h], joined(running[h], window[h]))

    @pl.loop(0, blocks)
    def _(b):
        at = pl.ds(pl.multiple_of(b * width, width), width)
        gate = jax.nn.sigmoid(proj[5, at, :].astype(F32))
        parts = []
        for h in range(heads):
            now = prefix[b, h]
            state = mm(now[:, :HEAD], window[h][:, HEAD:]) + now[:, HEAD:]
            read = reads[b, h]
            mixed = mm(read[:, :HEAD], state) + read[:, HEAD:]
            center = mixed - jnp.mean(mixed, axis=1, keepdims=True)
            spread = jnp.mean(center * center, axis=1, keepdims=True)
            parts.append(center * lax.rsqrt(spread + group_floor))
        gated[at, :] = (jnp.concatenate(parts, axis=1) * gain * gate).astype(BF16)

    def part(q):
        dest = lax.rem(t + q, m)
        rows = pl.ds(pl.multiple_of(dest * share, share), share)
        return remote(gated.at[rows, :], act.at[t], a_send.at[q], a_recv.at[q], s, dest)

    for q in range(1, m):
        part(q).start()
    act[t] = gated[pl.ds(pl.multiple_of(t * share, share), share), :]
    out_load.wait()
    for q in range(1, m):
        part(q).wait_recv()
    rows = jnp.concatenate([act[q] for q in range(m)], axis=1)
    columns = out_ref.shape[1]
    out_tile = min(512, columns)
    for c in range(0, columns, out_tile):
        out_ref[:, c : c + out_tile] = dot1(rows, wout[:, c : c + out_tile], NN).astype(BF16)
    for q in range(1, m):
        part(q).wait_send()
    for q in range(half):
        token_copy(q).wait_send()
    for q in range(1, half):
        forward_copy(q).wait_send()

    @pl.when(has_next)
    def _():
        for q in range(m):
            edge_copy(q).wait_send()

    @pl.when(has_middle)
    def _():
        for q in range(half):
            middle_copy(q).wait_send()

    for k, d in enumerate(steps):

        @pl.when(s + d < n)
        def _():
            hop(k).wait_send()


def per_device(
    n,
    m,
    tokens,
    norm_gain,
    w_recept,
    w_key,
    w_value,
    w_decay,
    w_rate,
    w_gate,
    shift_mix,
    decay_base,
    rate_base,
    decay_drift,
    group_gain,
    initial_state,
    w_out,
):
    share, depth = tokens.shape
    width = w_recept.shape[1]
    seq = share * m
    span = share * m // 2
    heads, blocks = width // HEAD, seq // BLOCK
    hops = max(1, (n - 1).bit_length())
    lanes = 128
    vmem = pl.BlockSpec(memory_space=pltpu.VMEM)
    anywhere = pl.BlockSpec(memory_space=pl.ANY)
    dma = pltpu.SemaphoreType.DMA
    return pl.pallas_call(
        functools.partial(layer_kernel, n, m, heads, blocks),
        out_shape=jax.ShapeDtypeStruct((share, w_out.shape[1]), BF16),
        in_specs=[pl.BlockSpec(memory_space=pltpu.SMEM), anywhere, vmem]
        + [anywhere] * 6
        + [vmem] * 5
        + [anywhere],
        out_specs=vmem,
        scratch_shapes=[
            pltpu.VMEM((m, share, depth), BF16),
            pltpu.VMEM((depth // lanes, lanes), F32),
            pltpu.VMEM((2, depth // lanes, lanes), F32),
            pltpu.VMEM((span + 16, depth), BF16),
            pltpu.VMEM((6, depth, width), BF16),
            pltpu.VMEM((6, seq, width), BF16),
            pltpu.VMEM((3, 16, width), F32),
            pltpu.VMEM((3, 8, width), F32),
            pltpu.VMEM((blocks, heads, BLOCK, 2 * HEAD), F32),
            pltpu.VMEM((blocks, heads, HEAD, 2 * HEAD), F32),
            pltpu.VMEM((blocks, heads, HEAD, 2 * HEAD), F32),
            pltpu.VMEM((heads, HEAD, 2 * HEAD), F32),
            pltpu.VMEM((heads, HEAD, 2 * HEAD), F32),
            pltpu.VMEM((hops, heads, HEAD, 2 * HEAD), F32),
            pltpu.VMEM((hops, heads, HEAD, 2 * HEAD), F32),
            pltpu.VMEM((seq, width), BF16),
            pltpu.VMEM((m, share, width), BF16),
            pltpu.VMEM(w_out.shape, BF16),
            dma,
            dma((7,)),
            dma((m,)),
            dma((m,)),
            dma((m,)),
            dma((m,)),
            dma((m,)),
            dma((2,)),
            dma((hops,)),
            dma((hops,)),
            dma((m,)),
            dma((m,)),
        ],
        compiler_params=pltpu.CompilerParams(
            collective_id=1, has_side_effects=True, vmem_limit_bytes=60 * 1024 * 1024
        ),
        name="layer_kernel",
    )(
        decay_drift,
        tokens,
        norm_gain,
        w_recept,
        w_key,
        w_value,
        w_decay,
        w_rate,
        w_gate,
        shift_mix,
        decay_base,
        rate_base,
        group_gain,
        initial_state,
        w_out,
    )


def solution(mesh):
    return jax.shard_map(
        functools.partial(per_device, mesh.shape["sp"], mesh.shape["tp"]),
        mesh=mesh,
        in_specs=(
            P(("sp", "tp"), None),
            P(),
            P(None, "tp"),
            P(None, "tp"),
            P(None, "tp"),
            P(None, "tp"),
            P(None, "tp"),
            P(None, "tp"),
            P(None, "tp"),
            P("tp"),
            P("tp"),
            P("sp"),
            P("tp"),
            P("tp", None, None),
            P(),
        ),
        out_specs=P(("sp", "tp"), None),
        check_vma=False,
    )
```

```python
import functools

import jax
import jax.numpy as jnp
from jax import lax
from jax.experimental import pallas as pl
from jax.experimental.pallas import tpu as pltpu
from jax.sharding import PartitionSpec as P

HEAD = 64
BLOCK = 64
F32 = jnp.float32
BF16 = jnp.bfloat16

norm_floor = 0.5
group_floor = 1.0

NN = (((1,), (0,)), ((), ()))
NT = (((1,), (1,)), ((), ()))
TN = (((0,), (0,)), ((), ()))


def dot1(a, b, dims):
    return lax.dot_general(a, b, dims, preferred_element_type=F32)


def split(a):
    high = a.astype(BF16)
    return high, (a - high.astype(F32)).astype(BF16)


def mm(a, b, dims=NN):
    ah, al = split(a)
    bh, bl = split(b)
    return dot1(ah, bh, dims) + (dot1(ah, bl, dims) + dot1(al, bh, dims))


def mm1(a, b, dims=NN):
    return dot1(a.astype(BF16), b.astype(BF16), dims)


def mm2(a, b, dims=NN):
    ah, al = split(a)
    return dot1(ah, b, dims) + dot1(al, b, dims)


def sum_rows(a, ones):
    high, rest = split(a)
    mid, low = split(a - high.astype(F32))
    return dot1(ones, high, NN) + (dot1(ones, mid, NN) + dot1(ones, low, NN))


def chunks_of(share):
    return max(c for c in (1, 2, 3, 4) if share % (16 * c) == 0)


def layer_kernel(
    n,
    m,
    heads,
    blocks,
    drift_ref,
    tok_ref,
    ngain_ref,
    wr_ref,
    wk_ref,
    wv_ref,
    wd_ref,
    wa_ref,
    wg_ref,
    mix_ref,
    dbase_ref,
    rbase_ref,
    gain_ref,
    init_ref,
    wout_ref,
    out_ref,
    tok,
    edge_out,
    edge_in,
    normed,
    weights,
    proj,
    edges,
    last_row,
    reads,
    ups,
    stack,
    final_reads,
    gates,
    pieces,
    prefix,
    running,
    window,
    g_buf,
    r_buf,
    gated,
    act,
    wout,
    own_sem,
    w_sem,
    t_send,
    t_recv,
    x_send,
    x_recv,
    f_send,
    f_recv,
    e_send,
    e_recv,
    g_send,
    g_recv,
    a_send,
    a_recv,
):
    s = lax.axis_index("sp")
    t = lax.axis_index("tp")
    half = m // 2
    upper = t // half
    base = upper * half
    across = lax.rem(t + half, m)
    share, depth = tok_ref.shape
    lanes = edge_out.shape[1]
    width = BLOCK
    channels = heads * HEAD
    steps = []
    while (1 << len(steps)) < n:
        steps.append(1 << len(steps))

    def near(q):
        return base + lax.rem(t - base + q, half)

    own_load = pltpu.make_async_copy(tok_ref, tok.at[t], own_sem)
    own_load.start()
    sources = (wr_ref, wk_ref, wv_ref, wd_ref, wa_ref, wg_ref)
    loads = [
        pltpu.make_async_copy(ref, weights.at[j], w_sem.at[j]) for j, ref in enumerate(sources)
    ]
    for load in loads:
        load.start()
    out_load = pltpu.make_async_copy(wout_ref, wout, w_sem.at[len(sources)])
    out_load.start()

    barrier = pltpu.get_barrier_semaphore()
    count = m - 1

    def greet(sp, tp):
        pl.semaphore_signal(
            barrier, inc=1, device_id={"sp": sp, "tp": tp}, device_id_type=pl.DeviceIdType.MESH
        )

    for q in range(1, m):
        greet(s, lax.rem(t + q, m))
    for d in steps:
        for other, ok in ((s + d, s + d < n), (s - d, s - d >= 0)):
            count = count + ok.astype(jnp.int32)

            @pl.when(ok)
            def _():
                greet(other, t)

    for q in range(m - 1):
        sends = jnp.logical_and(t == m - 1, s + 1 < n)
        takes = jnp.logical_and(t == q, s >= 1)
        count = count + sends.astype(jnp.int32) + takes.astype(jnp.int32)

        @pl.when(sends)
        def _():
            greet(s + 1, q)

        @pl.when(takes)
        def _():
            greet(s - 1, m - 1)

    own_load.wait()
    last = tok[t, share - 16 :, :].astype(F32)[15:16, :]
    for i in range(depth // lanes):
        edge_out[i : i + 1, :] = last[:, i * lanes : (i + 1) * lanes]
    pl.semaphore_wait(barrier, count)

    def remote(src, dst, send, recv, sp, tp):
        return pltpu.make_async_remote_copy(
            src_ref=src,
            dst_ref=dst,
            send_sem=send,
            recv_sem=recv,
            device_id={"sp": sp, "tp": tp},
            device_id_type=pl.DeviceIdType.MESH,
        )

    def token_copy(q):
        return remote(tok.at[t], tok.at[t], t_send.at[q], t_recv.at[q], s, near(q))

    chunks = chunks_of(share)
    rows_each = share // chunks

    def across_copy(c):
        some = tok.at[t, pl.ds(c * rows_each, rows_each), :]
        return remote(some, some, x_send.at[c], x_recv.at[c], s, across)

    def forward_copy(q, c):
        some = tok.at[across, pl.ds(c * rows_each, rows_each), :]
        return remote(some, some, f_send.at[q, c], f_recv.at[q, c], s, near(q))

    def edge_copy(q):
        return remote(edge_out, edge_in.at[0], e_send.at[q], e_recv.at[0], s + 1, q)

    def middle_copy(q):
        return remote(edge_out, edge_in.at[1], e_send.at[q], e_recv.at[1], s, half + q)

    has_next = jnp.logical_and(t == m - 1, s + 1 < n)
    has_middle = t == half - 1

    @pl.when(has_next)
    def _():
        for q in range(m):
            edge_copy(q).start()

    @pl.when(has_middle)
    def _():
        for q in range(half):
            middle_copy(q).start()

    for c in range(chunks):
        across_copy(c).start()
    for q in range(1, half):
        token_copy(q).start()

    rows_i = lax.broadcasted_iota(jnp.int32, (width, width), 0)
    cols_i = lax.broadcasted_iota(jnp.int32, (width, width), 1)
    strict = cols_i < rows_i
    incl = cols_i <= rows_i
    eye = jnp.where(cols_i == rows_i, 1.0, 0.0).astype(F32)
    ones = jnp.where(incl, 1.0, 0.0).astype(BF16)
    incl_two = jnp.concatenate([jnp.where(incl, 1.0, 0.0)] * 2, axis=1) > 0.5
    zeros = jnp.zeros((width, HEAD), F32)
    levels = []
    size = 1
    while size < width:
        same = (rows_i // (2 * size)) == (cols_i // (2 * size))
        levels.append(same & ((rows_i // size) % 2 == 1) & ((cols_i // size) % 2 == 0))
        size *= 2
    first_row = lax.broadcasted_iota(jnp.int32, (width, channels), 0) == 0
    mix = mix_ref[...]
    dbase = dbase_ref[...].reshape(1, channels)
    rbase = rbase_ref[...].reshape(1, channels)
    gain = gain_ref[...].reshape(1, channels)
    ngain = ngain_ref[...].reshape(1, depth)

    def norm(x):
        scale = lax.rsqrt(jnp.mean(x * x, axis=1, keepdims=True) + norm_floor)
        return (x * scale * ngain).astype(BF16)

    tile = 16
    span = half * share

    def norm_block(owner, place, begin=0, number=share):
        @pl.loop(0, number // tile)
        def _(i):
            rows = pl.ds(pl.multiple_of(begin + i * tile, tile), tile)
            to = pl.ds(pl.multiple_of(place * share + begin + i * tile, tile), tile)
            normed[to, :] = norm(tok[owner, rows, :].astype(F32))

    def project(first, extra):
        to = pl.ds(pl.multiple_of(first * share, share), span)
        for j in range(len(sources)):
            if extra:
                loads[j].wait()
            if extra and j < 3:
                made = dot1(normed[...], weights[j], NN).astype(BF16)
                edges[j] = made[span:, :].astype(F32)
                proj[j, to, :] = made[:span, :]
            else:
                proj[j, to, :] = dot1(normed[:span, :], weights[j], NN).astype(BF16)

    def prepare(bs):
        units, alphas, betas, keys, vals, fins, cross, recs = [], [], [], [], [], [], [], []
        for b in bs:
            at = pl.ds(pl.multiple_of(b * width, width), width)

            def shifted(j):
                cur = proj[j, at, :].astype(F32)
                earlier = jnp.where(first_row, last_row[j, 0:1, :], pltpu.roll(cur, 1, 0))
                last_row[j] = jnp.broadcast_to(cur[width - 1 :, :], (8, channels))
                return cur + (earlier - cur) * mix[j : j + 1, :]

            recept, key, value = shifted(0), shifted(1), shifted(2)
            level = dbase + proj[3, at, :].astype(F32) + drift_ref[b * width]
            logs = -0.6065306597126334 * jax.nn.sigmoid(level)
            rate = jax.nn.sigmoid(rbase + proj[4, at, :].astype(F32))
            total = sum_rows(logs, ones)
            through = jnp.exp(total)
            until = jnp.exp(total - logs)
            inverse = jnp.exp(-total)
            key_s = key * inverse
            rec_s = recept * through
            final = through[width - 1 :, :]
            rate_inv = rate * inverse
            for h in range(heads):
                ch = slice(h * HEAD, (h + 1) * HEAD)
                key_h = key[:, ch]
                unit = key_h * lax.rsqrt(jnp.sum(key_h * key_h, axis=1, keepdims=True) + 1.0)
                units.append((b, h))
                alphas.append(-unit * until[:, ch])
                betas.append(unit * rate_inv[:, ch])
                keys.append(key_s[:, ch])
                vals.append(value[:, ch])
                fins.append(final[:, ch])
                recs.append(rec_s[:, ch])
                reads[b, h, :, :HEAD] = rec_s[:, ch]
        every = range(len(units))
        cross = [
            mm(
                jnp.concatenate([alphas[u], recs[u]], axis=0),
                jnp.concatenate([betas[u], keys[u]], axis=0),
                NT,
            )
            for u in every
        ]
        for u in every:
            ups[units[u]] = jnp.where(incl_two, cross[u][width:, :], 0.0).astype(BF16)
        low_ab = [jnp.where(strict, c[:width, :width], 0.0) for c in cross]
        low_ak = [jnp.where(strict, c[:width, width:], 0.0) for c in cross]
        both = [mm(low_ak[u], vals[u]) for u in every]
        inv = [eye + jnp.where(levels[0], low, 0.0) for low in low_ab]
        for mask in levels[1:]:
            short = [i.astype(BF16) for i in inv]
            right = [mm1(jnp.where(mask, low_ab[u], 0.0), short[u]) for u in every]
            inv = [inv[u] + mm1(short[u], right[u]) for u in every]
        solved = [mm(inv[u], jnp.concatenate([alphas[u], both[u]], axis=1)) for u in every]
        for u in every:
            ends = jnp.concatenate([betas[u] * fins[u], keys[u] * fins[u]], axis=0)
            column = jnp.concatenate(
                [solved[u], jnp.concatenate([zeros, vals[u]], axis=1)], axis=0
            )
            stack[units[u]] = column.astype(BF16)
            pieces[units[u]] = mm(ends, column, TN) + jnp.concatenate(
                [eye * fins[u], zeros], axis=1
            )

    def centered(x):
        return x - jnp.mean(x, axis=1, keepdims=True)

    def defer(b):
        at = pl.ds(pl.multiple_of(b * width, width), width)
        for h in range(heads):
            made = dot1(ups[b, h], stack[b, h], NN)
            read = reads[b, h, :, :HEAD] + made[:, :HEAD]
            both = mm(read, prefix[b, h])
            fixed = centered(both[:, HEAD:] + made[:, HEAD:])
            final_reads[h, at, :] = jnp.concatenate([both[:, :HEAD], fixed], axis=1)
        gates[at, :] = jax.nn.sigmoid(proj[5, at, :].astype(F32)) * gain

    def open_half(which):
        for j in range(3):
            row = jnp.where(which == 0, edges[j, 0:1, :], edges[j, 1:2, :])
            last_row[j] = jnp.broadcast_to(row, (8, channels))

    norm_block(t, t - base)
    for q in range(1, half):
        token_copy(q).wait_recv()
        norm_block(near(half - q), near(half - q) - base)

    @pl.when(s >= 1)
    def _():
        remote(edge_out, edge_in.at[0], e_send.at[0], e_recv.at[0], s, t).wait_recv()

    @pl.when(s == 0)
    def _():
        edge_in[0] = jnp.zeros(edge_in.shape[1:], F32)

    @pl.when(upper == 1)
    def _():
        remote(edge_out, edge_in.at[1], e_send.at[0], e_recv.at[1], s, t).wait_recv()

    @pl.when(upper == 0)
    def _():
        row = tok[half - 1, share - 16 :, :].astype(F32)[15:16, :]
        for i in range(depth // lanes):
            edge_in[1, i : i + 1, :] = row[:, i * lanes : (i + 1) * lanes]

    joined_rows = [
        jnp.concatenate([edge_in[k, i : i + 1, :] for i in range(depth // lanes)], axis=1)
        for k in range(2)
    ]
    normed[span:, :] = norm(
        jnp.concatenate(joined_rows + [jnp.zeros((14, depth), F32)], axis=0)
    )
    project(base, True)
    open_half(upper)

    group = max(g for g in (1, 2, 3) if (blocks // 2) % g == 0)

    def prepare_half(first):
        @pl.loop(0, blocks // 2 // group)
        def _(i):
            prepare([first + i * group + g for g in range(group)])

    prepare_half(upper * (blocks // 2))

    lower = 1 - upper
    for c in range(chunks):
        across_copy(c).wait_recv()
        for q in range(1, half):
            forward_copy(q, c).start()
        norm_block(across, across - lower * half, c * rows_each, rows_each)
    for q in range(1, half):
        far = lower * half + near(half - q) - base
        for c in range(chunks):
            forward_copy(q, c).wait_recv()
            norm_block(far, far - lower * half, c * rows_each, rows_each)
    project(lower * half, False)
    open_half(lower)

    prepare_half(lower * (blocks // 2))

    def joined(later, earlier):
        return mm(later[:, :HEAD], earlier) + jnp.concatenate([zeros, later[:, HEAD:]], axis=1)

    for h in range(heads):
        running[h] = jnp.concatenate([eye, zeros], axis=1)

    @pl.loop(0, blocks)
    def _(b):
        for h in range(heads):
            prefix[b, h] = running[h]
            running[h] = joined(pieces[b, h], running[h])

    at_start = s == 0
    for h in range(heads):
        own = running[h]
        start = jnp.concatenate([zeros, init_ref[h].T], axis=1)
        window[h] = jnp.where(at_start, start, jnp.concatenate([eye, zeros], axis=1))
        whole = jnp.where(at_start, joined(own, start), own)
        running[h] = whole
        g_buf[0, h] = whole.astype(BF16)

    def hop(k):
        return remote(g_buf.at[k], r_buf.at[k], g_send.at[k], g_recv.at[k], s + steps[k], t)

    for k, d in enumerate(steps):

        @pl.when(s + d < n)
        def _():
            hop(k).start()

        @pl.loop(k * blocks // len(steps), (k + 1) * blocks // len(steps))
        def _(b):
            defer(b)

        @pl.when(s - d >= 0)
        def _():
            hop(k).wait_recv()
            for h in range(heads):
                now = window[h]
                window[h] = mm2(now[:, :HEAD], r_buf[k, h]) + jnp.concatenate(
                    [zeros, now[:, HEAD:]], axis=1
                )

        if k + 1 < len(steps):
            for h in range(heads):
                whole = jnp.where(at_start, running[h], joined(running[h], window[h]))
                g_buf[k + 1, h] = whole.astype(BF16)

    entry = [split(centered(window[h][:, HEAD:])) for h in range(heads)]

    def finish(dest):
        at = pl.ds(pl.multiple_of(dest * share, share), share)
        parts = []
        for h in range(heads):
            read = final_reads[h, at, :]
            high, low = split(read[:, :HEAD])
            center = dot1(high, entry[h][0], NN) + (
                dot1(high, entry[h][1], NN) + dot1(low, entry[h][0], NN)
            )
            center = center + read[:, HEAD:]
            spread = jnp.mean(center * center, axis=1, keepdims=True)
            parts.append(center * lax.rsqrt(spread + group_floor))
        return (jnp.concatenate(parts, axis=1) * gates[at, :]).astype(BF16)

    def part(q):
        dest = lax.rem(t + q, m)
        return remote(gated.at[q - 1], act.at[t], a_send.at[q], a_recv.at[q], s, dest)

    for q in range(1, m):
        gated[q - 1] = finish(lax.rem(t + q, m))
        part(q).start()
    act[t] = finish(t)
    out_load.wait()
    for q in range(1, m):
        part(q).wait_recv()
    rows = jnp.concatenate([act[q] for q in range(m)], axis=1)
    columns = out_ref.shape[1]
    out_tile = min(512, columns)
    for c in range(0, columns, out_tile):
        out_ref[:, c : c + out_tile] = dot1(rows, wout[:, c : c + out_tile], NN).astype(BF16)
    for q in range(1, m):
        part(q).wait_send()
    for c in range(chunks):
        across_copy(c).wait_send()
    for q in range(1, half):
        token_copy(q).wait_send()
        for c in range(chunks):
            forward_copy(q, c).wait_send()

    @pl.when(has_next)
    def _():
        for q in range(m):
            edge_copy(q).wait_send()

    @pl.when(has_middle)
    def _():
        for q in range(half):
            middle_copy(q).wait_send()

    for k, d in enumerate(steps):

        @pl.when(s + d < n)
        def _():
            hop(k).wait_send()


def per_device(
    n,
    m,
    tokens,
    norm_gain,
    w_recept,
    w_key,
    w_value,
    w_decay,
    w_rate,
    w_gate,
    shift_mix,
    decay_base,
    rate_base,
    decay_drift,
    group_gain,
    initial_state,
    w_out,
):
    share, depth = tokens.shape
    width = w_recept.shape[1]
    seq = share * m
    span = share * m // 2
    heads, blocks = width // HEAD, seq // BLOCK
    hops = max(1, (n - 1).bit_length())
    lanes = 128
    vmem = pl.BlockSpec(memory_space=pltpu.VMEM)
    anywhere = pl.BlockSpec(memory_space=pl.ANY)
    dma = pltpu.SemaphoreType.DMA
    return pl.pallas_call(
        functools.partial(layer_kernel, n, m, heads, blocks),
        out_shape=jax.ShapeDtypeStruct((share, w_out.shape[1]), BF16),
        in_specs=[pl.BlockSpec(memory_space=pltpu.SMEM), anywhere, vmem]
        + [anywhere] * 6
        + [vmem] * 5
        + [anywhere],
        out_specs=vmem,
        scratch_shapes=[
            pltpu.VMEM((m, share, depth), BF16),
            pltpu.VMEM((depth // lanes, lanes), F32),
            pltpu.VMEM((2, depth // lanes, lanes), F32),
            pltpu.VMEM((span + 16, depth), BF16),
            pltpu.VMEM((6, depth, width), BF16),
            pltpu.VMEM((6, seq, width), BF16),
            pltpu.VMEM((3, 16, width), F32),
            pltpu.VMEM((3, 8, width), F32),
            pltpu.VMEM((blocks, heads, BLOCK, 2 * HEAD), F32),
            pltpu.VMEM((blocks, heads, BLOCK, 2 * HEAD), BF16),
            pltpu.VMEM((blocks, heads, 2 * BLOCK, 2 * HEAD), BF16),
            pltpu.VMEM((heads, seq, 2 * HEAD), F32),
            pltpu.VMEM((seq, width), F32),
            pltpu.VMEM((blocks, heads, HEAD, 2 * HEAD), F32),
            pltpu.VMEM((blocks, heads, HEAD, 2 * HEAD), F32),
            pltpu.VMEM((heads, HEAD, 2 * HEAD), F32),
            pltpu.VMEM((heads, HEAD, 2 * HEAD), F32),
            pltpu.VMEM((hops, heads, HEAD, 2 * HEAD), BF16),
            pltpu.VMEM((hops, heads, HEAD, 2 * HEAD), BF16),
            pltpu.VMEM((m - 1, share, width), BF16),
            pltpu.VMEM((m, share, width), BF16),
            pltpu.VMEM(w_out.shape, BF16),
            dma,
            dma((7,)),
            dma((m,)),
            dma((m,)),
            dma((chunks_of(share),)),
            dma((chunks_of(share),)),
            dma((m, chunks_of(share))),
            dma((m, chunks_of(share))),
            dma((m,)),
            dma((2,)),
            dma((hops,)),
            dma((hops,)),
            dma((m,)),
            dma((m,)),
        ],
        compiler_params=pltpu.CompilerParams(
            collective_id=1, has_side_effects=True, vmem_limit_bytes=60 * 1024 * 1024
        ),
        name="layer_kernel",
    )(
        decay_drift,
        tokens,
        norm_gain,
        w_recept,
        w_key,
        w_value,
        w_decay,
        w_rate,
        w_gate,
        shift_mix,
        decay_base,
        rate_base,
        group_gain,
        initial_state,
        w_out,
    )


def solution(mesh):
    return jax.shard_map(
        functools.partial(per_device, mesh.shape["sp"], mesh.shape["tp"]),
        mesh=mesh,
        in_specs=(
            P(("sp", "tp"), None),
            P(),
            P(None, "tp"),
            P(None, "tp"),
            P(None, "tp"),
            P(None, "tp"),
            P(None, "tp"),
            P(None, "tp"),
            P(None, "tp"),
            P("tp"),
            P("tp"),
            P("sp"),
            P("tp"),
            P("tp", None, None),
            P(),
        ),
        out_specs=P(("sp", "tp"), None),
        check_vma=False,
    )
```

```python
import functools

import jax
import jax.numpy as jnp
from jax import lax
from jax.experimental import pallas as pl
from jax.experimental.pallas import tpu as pltpu
from jax.sharding import PartitionSpec as P

HEAD = 64
BLOCK = 64
F32 = jnp.float32
BF16 = jnp.bfloat16

norm_floor = 0.5
group_floor = 1.0

NN = (((1,), (0,)), ((), ()))
NT = (((1,), (1,)), ((), ()))
TN = (((0,), (0,)), ((), ()))


def dot1(a, b, dims):
    return lax.dot_general(a, b, dims, preferred_element_type=F32)


def split(a):
    high = a.astype(BF16)
    return high, (a - high.astype(F32)).astype(BF16)


def mm(a, b, dims=NN):
    ah, al = split(a)
    bh, bl = split(b)
    return dot1(ah, bh, dims) + (dot1(ah, bl, dims) + dot1(al, bh, dims))


def mm1(a, b, dims=NN):
    return dot1(a.astype(BF16), b.astype(BF16), dims)


def mm2(a, b, dims=NN):
    ah, al = split(a)
    return dot1(ah, b, dims) + dot1(al, b, dims)


def sum_rows(a, ones):
    high, rest = split(a)
    mid, low = split(a - high.astype(F32))
    return dot1(ones, high, NN) + (dot1(ones, mid, NN) + dot1(ones, low, NN))


def chunks_of(share):
    return max(c for c in (1, 2, 3, 4) if share % (16 * c) == 0)


def layer_kernel(
    n,
    m,
    heads,
    blocks,
    drift_ref,
    tok_ref,
    ngain_ref,
    wr_ref,
    wk_ref,
    wv_ref,
    wd_ref,
    wa_ref,
    wg_ref,
    mix_ref,
    dbase_ref,
    rbase_ref,
    gain_ref,
    init_ref,
    wout_ref,
    out_ref,
    tok,
    edge_out,
    edge_in,
    normed,
    weights,
    proj,
    edges,
    last_row,
    reads,
    ups,
    stack,
    final_reads,
    gates,
    pieces,
    prefix,
    running,
    window,
    g_buf,
    r_buf,
    c_out,
    c_in,
    gated,
    act,
    wout,
    own_sem,
    w_sem,
    t_send,
    t_recv,
    x_send,
    x_recv,
    f_send,
    f_recv,
    e_send,
    e_recv,
    g_send,
    g_recv,
    a_send,
    a_recv,
):
    s = lax.axis_index("sp")
    t = lax.axis_index("tp")
    half = m // 2
    upper = t // half
    base = upper * half
    across = lax.rem(t + half, m)
    share, depth = tok_ref.shape
    lanes = edge_out.shape[1]
    width = BLOCK
    channels = heads * HEAD
    steps = []
    while (1 << len(steps)) < n:
        steps.append(1 << len(steps))

    def near(q):
        return base + lax.rem(t - base + q, half)

    own_load = pltpu.make_async_copy(tok_ref, tok.at[t], own_sem)
    own_load.start()
    sources = (wr_ref, wk_ref, wv_ref, wd_ref, wa_ref, wg_ref)
    loads = [
        pltpu.make_async_copy(ref, weights.at[j], w_sem.at[j]) for j, ref in enumerate(sources)
    ]
    for load in loads:
        load.start()
    out_load = pltpu.make_async_copy(wout_ref, wout, w_sem.at[len(sources)])

    barrier = pltpu.get_barrier_semaphore()
    count = m - 1

    def greet(sp, tp):
        pl.semaphore_signal(
            barrier, inc=1, device_id={"sp": sp, "tp": tp}, device_id_type=pl.DeviceIdType.MESH
        )

    for q in range(1, m):
        greet(s, lax.rem(t + q, m))
    for d in steps:
        for other, ok in ((s + d, s + d < n), (s - d, s - d >= 0)):
            count = count + ok.astype(jnp.int32)

            @pl.when(ok)
            def _():
                greet(other, t)

    for q in range(m - 1):
        sends = jnp.logical_and(t == m - 1, s + 1 < n)
        takes = jnp.logical_and(t == q, s >= 1)
        count = count + sends.astype(jnp.int32) + takes.astype(jnp.int32)

        @pl.when(sends)
        def _():
            greet(s + 1, q)

        @pl.when(takes)
        def _():
            greet(s - 1, m - 1)

    own_load.wait()
    last = tok[t, share - 16 :, :].astype(F32)[15:16, :]
    for i in range(depth // lanes):
        edge_out[i : i + 1, :] = last[:, i * lanes : (i + 1) * lanes]
    pl.semaphore_wait(barrier, count)

    def remote(src, dst, send, recv, sp, tp):
        return pltpu.make_async_remote_copy(
            src_ref=src,
            dst_ref=dst,
            send_sem=send,
            recv_sem=recv,
            device_id={"sp": sp, "tp": tp},
            device_id_type=pl.DeviceIdType.MESH,
        )

    def token_copy(q):
        return remote(tok.at[t], tok.at[t], t_send.at[q], t_recv.at[q], s, near(q))

    chunks = chunks_of(share)
    rows_each = share // chunks

    def across_copy(c):
        some = tok.at[t, pl.ds(c * rows_each, rows_each), :]
        return remote(some, some, x_send.at[c], x_recv.at[c], s, across)

    def forward_copy(q, c):
        some = tok.at[across, pl.ds(c * rows_each, rows_each), :]
        return remote(some, some, f_send.at[q, c], f_recv.at[q, c], s, near(q))

    def edge_copy(q):
        return remote(edge_out, edge_in.at[0], e_send.at[q], e_recv.at[0], s + 1, q)

    def middle_copy(q):
        return remote(edge_out, edge_in.at[1], e_send.at[q], e_recv.at[1], s, half + q)

    has_next = jnp.logical_and(t == m - 1, s + 1 < n)
    has_middle = t == half - 1

    @pl.when(has_next)
    def _():
        for q in range(m):
            edge_copy(q).start()

    @pl.when(has_middle)
    def _():
        for q in range(half):
            middle_copy(q).start()

    for c in range(chunks):
        across_copy(c).start()
    for q in range(1, half):
        token_copy(q).start()

    rows_i = lax.broadcasted_iota(jnp.int32, (width, width), 0)
    cols_i = lax.broadcasted_iota(jnp.int32, (width, width), 1)
    strict = cols_i < rows_i
    incl = cols_i <= rows_i
    eye = jnp.where(cols_i == rows_i, 1.0, 0.0).astype(F32)
    ones = jnp.where(incl, 1.0, 0.0).astype(BF16)
    incl_two = jnp.concatenate([jnp.where(incl, 1.0, 0.0)] * 2, axis=1) > 0.5
    zeros = jnp.zeros((width, HEAD), F32)
    levels = []
    size = 1
    while size < width:
        same = (rows_i // (2 * size)) == (cols_i // (2 * size))
        levels.append(same & ((rows_i // size) % 2 == 1) & ((cols_i // size) % 2 == 0))
        size *= 2
    first_row = lax.broadcasted_iota(jnp.int32, (width, channels), 0) == 0
    mix = mix_ref[...]
    dbase = dbase_ref[...].reshape(1, channels)
    rbase = rbase_ref[...].reshape(1, channels)
    gain = gain_ref[...].reshape(1, channels)
    ngain = ngain_ref[...].reshape(1, depth)

    def norm(x):
        scale = lax.rsqrt(jnp.mean(x * x, axis=1, keepdims=True) + norm_floor)
        return (x * scale * ngain).astype(BF16)

    tile = 16
    span = half * share

    def norm_block(owner, place, begin=0, number=share):
        @pl.loop(0, number // tile)
        def _(i):
            rows = pl.ds(pl.multiple_of(begin + i * tile, tile), tile)
            to = pl.ds(pl.multiple_of(place * share + begin + i * tile, tile), tile)
            normed[to, :] = norm(tok[owner, rows, :].astype(F32))

    def project(first, extra):
        to = pl.ds(pl.multiple_of(first * share, share), span)
        for j in range(len(sources)):
            if extra:
                loads[j].wait()
            if extra and j < 3:
                made = dot1(normed[...], weights[j], NN).astype(BF16)
                edges[j] = made[span:, :].astype(F32)
                proj[j, to, :] = made[:span, :]
            else:
                proj[j, to, :] = dot1(normed[:span, :], weights[j], NN).astype(BF16)

    def prepare(bs):
        units, alphas, betas, keys, vals, fins, cross, recs = [], [], [], [], [], [], [], []
        for b in bs:
            at = pl.ds(pl.multiple_of(b * width, width), width)

            def shifted(j):
                cur = proj[j, at, :].astype(F32)
                earlier = jnp.where(first_row, last_row[j, 0:1, :], pltpu.roll(cur, 1, 0))
                last_row[j] = jnp.broadcast_to(cur[width - 1 :, :], (8, channels))
                return cur + (earlier - cur) * mix[j : j + 1, :]

            recept, key, value = shifted(0), shifted(1), shifted(2)
            level = dbase + proj[3, at, :].astype(F32) + drift_ref[b * width]
            logs = -0.6065306597126334 * jax.nn.sigmoid(level)
            rate = jax.nn.sigmoid(rbase + proj[4, at, :].astype(F32))
            total = sum_rows(logs, ones)
            through = jnp.exp(total)
            until = jnp.exp(total - logs)
            inverse = jnp.exp(-total)
            key_s = key * inverse
            rec_s = recept * through
            final = through[width - 1 :, :]
            rate_inv = rate * inverse
            for h in range(heads):
                ch = slice(h * HEAD, (h + 1) * HEAD)
                key_h = key[:, ch]
                unit = key_h * lax.rsqrt(jnp.sum(key_h * key_h, axis=1, keepdims=True) + 1.0)
                units.append((b, h))
                alphas.append(-unit * until[:, ch])
                betas.append(unit * rate_inv[:, ch])
                keys.append(key_s[:, ch])
                vals.append(value[:, ch])
                fins.append(final[:, ch])
                recs.append(rec_s[:, ch])
                reads[b, h, :, :HEAD] = rec_s[:, ch]
        every = range(len(units))
        cross = [
            mm(
                jnp.concatenate([alphas[u], recs[u]], axis=0),
                jnp.concatenate([betas[u], keys[u]], axis=0),
                NT,
            )
            for u in every
        ]
        for u in every:
            ups[units[u]] = jnp.where(incl_two, cross[u][width:, :], 0.0).astype(BF16)
        low_ab = [jnp.where(strict, c[:width, :width], 0.0) for c in cross]
        low_ak = [jnp.where(strict, c[:width, width:], 0.0) for c in cross]
        both = [mm(low_ak[u], vals[u]) for u in every]
        inv = [eye + jnp.where(levels[0], low, 0.0) for low in low_ab]
        for mask in levels[1:]:
            short = [i.astype(BF16) for i in inv]
            right = [mm1(jnp.where(mask, low_ab[u], 0.0), short[u]) for u in every]
            inv = [inv[u] + mm1(short[u], right[u]) for u in every]
        solved = [mm(inv[u], jnp.concatenate([alphas[u], both[u]], axis=1)) for u in every]
        for u in every:
            ends = jnp.concatenate([betas[u] * fins[u], keys[u] * fins[u]], axis=0)
            column = jnp.concatenate(
                [solved[u], jnp.concatenate([zeros, vals[u]], axis=1)], axis=0
            )
            stack[units[u]] = column.astype(BF16)
            pieces[units[u]] = mm(ends, column, TN) + jnp.concatenate(
                [eye * fins[u], zeros], axis=1
            )

    def centered(x):
        return x - jnp.mean(x, axis=1, keepdims=True)

    def defer(b):
        at = pl.ds(pl.multiple_of(b * width, width), width)
        for h in range(heads):
            made = dot1(ups[b, h], stack[b, h], NN)
            read = reads[b, h, :, :HEAD] + made[:, :HEAD]
            both = mm(read, prefix[b, h])
            fixed = centered(both[:, HEAD:] + made[:, HEAD:])
            final_reads[h, at, :] = jnp.concatenate([both[:, :HEAD], fixed], axis=1)
        gates[at, :] = jax.nn.sigmoid(proj[5, at, :].astype(F32)) * gain

    def open_half(which):
        for j in range(3):
            row = jnp.where(which == 0, edges[j, 0:1, :], edges[j, 1:2, :])
            last_row[j] = jnp.broadcast_to(row, (8, channels))

    norm_block(t, t - base)
    for q in range(1, half):
        token_copy(q).wait_recv()
        norm_block(near(half - q), near(half - q) - base)

    @pl.when(s >= 1)
    def _():
        remote(edge_out, edge_in.at[0], e_send.at[0], e_recv.at[0], s, t).wait_recv()

    @pl.when(s == 0)
    def _():
        edge_in[0] = jnp.zeros(edge_in.shape[1:], F32)

    @pl.when(upper == 1)
    def _():
        remote(edge_out, edge_in.at[1], e_send.at[0], e_recv.at[1], s, t).wait_recv()

    @pl.when(upper == 0)
    def _():
        row = tok[half - 1, share - 16 :, :].astype(F32)[15:16, :]
        for i in range(depth // lanes):
            edge_in[1, i : i + 1, :] = row[:, i * lanes : (i + 1) * lanes]

    joined_rows = [
        jnp.concatenate([edge_in[k, i : i + 1, :] for i in range(depth // lanes)], axis=1)
        for k in range(2)
    ]
    normed[span:, :] = norm(
        jnp.concatenate(joined_rows + [jnp.zeros((14, depth), F32)], axis=0)
    )
    project(base, True)
    out_load.start()
    open_half(upper)

    group = max(g for g in (1, 2, 3) if (blocks // 2) % g == 0)

    def prepare_half(first):
        @pl.loop(0, blocks // 2 // group)
        def _(i):
            prepare([first + i * group + g for g in range(group)])

    prepare_half(upper * (blocks // 2))

    lower = 1 - upper
    for c in range(chunks):
        across_copy(c).wait_recv()
        for q in range(1, half):
            forward_copy(q, c).start()
        norm_block(across, across - lower * half, c * rows_each, rows_each)
    for q in range(1, half):
        far = lower * half + near(half - q) - base
        for c in range(chunks):
            forward_copy(q, c).wait_recv()
            norm_block(far, far - lower * half, c * rows_each, rows_each)
    project(lower * half, False)
    open_half(lower)

    prepare_half(lower * (blocks // 2))

    def joined(later, earlier):
        return mm(later[:, :HEAD], earlier) + jnp.concatenate([zeros, later[:, HEAD:]], axis=1)

    for h in range(heads):
        running[h] = jnp.concatenate([eye, zeros], axis=1)

    @pl.loop(0, blocks)
    def _(b):
        for h in range(heads):
            prefix[b, h] = running[h]
            running[h] = joined(pieces[b, h], running[h])

    at_start = s == 0
    for h in range(heads):
        own = running[h]
        start = jnp.concatenate([zeros, init_ref[h].T], axis=1)
        window[h] = jnp.where(at_start, start, jnp.concatenate([eye, zeros], axis=1))
        whole = jnp.where(at_start, joined(own, start), own)
        running[h] = whole

    final_hop = len(steps) - 1

    def offer(k, wholes):
        if k < final_hop:
            for h in range(heads):
                g_buf[k, h] = wholes[h].astype(BF16)
        else:
            for p in range(heads // 2):
                pair = [wholes[2 * p][:, HEAD:], wholes[2 * p + 1][:, HEAD:]]
                c_out[p] = jnp.concatenate(pair, axis=1).astype(BF16)

    offer(0, [running[h] for h in range(heads)])

    def hop(k):
        src, dst = (g_buf.at[k], r_buf.at[k]) if k < final_hop else (c_out, c_in)
        return remote(src, dst, g_send.at[k], g_recv.at[k], s + steps[k], t)

    for k, d in enumerate(steps):

        @pl.when(s + d < n)
        def _():
            hop(k).start()

        @pl.loop(k * blocks // len(steps), (k + 1) * blocks // len(steps))
        def _(b):
            defer(b)

        @pl.when(s - d >= 0)
        def _():
            hop(k).wait_recv()
            for h in range(heads):
                now = window[h]
                if k < final_hop:
                    window[h] = mm2(now[:, :HEAD], r_buf[k, h]) + jnp.concatenate(
                        [zeros, now[:, HEAD:]], axis=1
                    )
                else:
                    lane = (h % 2) * HEAD
                    got = mm2(now[:, :HEAD], c_in[h // 2])[:, lane : lane + HEAD]
                    window[h] = jnp.concatenate([zeros, got + now[:, HEAD:]], axis=1)

        if k + 1 < len(steps):
            offer(
                k + 1,
                [
                    jnp.where(at_start, running[h], joined(running[h], window[h]))
                    for h in range(heads)
                ],
            )

    entry = [split(centered(window[h][:, HEAD:])) for h in range(heads)]

    def finish(dest):
        at = pl.ds(pl.multiple_of(dest * share, share), share)
        parts = []
        for h in range(heads):
            read = final_reads[h, at, :]
            high, low = split(read[:, :HEAD])
            center = dot1(high, entry[h][0], NN) + (
                dot1(high, entry[h][1], NN) + dot1(low, entry[h][0], NN)
            )
            center = center + read[:, HEAD:]
            spread = jnp.mean(center * center, axis=1, keepdims=True)
            parts.append(center * lax.rsqrt(spread + group_floor))
        return (jnp.concatenate(parts, axis=1) * gates[at, :]).astype(BF16)

    def part(q):
        dest = lax.rem(t + q, m)
        return remote(gated.at[q - 1], act.at[t], a_send.at[q], a_recv.at[q], s, dest)

    for q in range(1, m):
        gated[q - 1] = finish(lax.rem(t + q, m))
        part(q).start()
    act[t] = finish(t)
    out_load.wait()
    for q in range(1, m):
        part(q).wait_recv()
    rows = jnp.concatenate([act[q] for q in range(m)], axis=1)
    columns = out_ref.shape[1]
    out_tile = min(512, columns)
    for c in range(0, columns, out_tile):
        out_ref[:, c : c + out_tile] = dot1(rows, wout[:, c : c + out_tile], NN).astype(BF16)
    for q in range(1, m):
        part(q).wait_send()
    for c in range(chunks):
        across_copy(c).wait_send()
    for q in range(1, half):
        token_copy(q).wait_send()
        for c in range(chunks):
            forward_copy(q, c).wait_send()

    @pl.when(has_next)
    def _():
        for q in range(m):
            edge_copy(q).wait_send()

    @pl.when(has_middle)
    def _():
        for q in range(half):
            middle_copy(q).wait_send()

    for k, d in enumerate(steps):

        @pl.when(s + d < n)
        def _():
            hop(k).wait_send()


def per_device(
    n,
    m,
    tokens,
    norm_gain,
    w_recept,
    w_key,
    w_value,
    w_decay,
    w_rate,
    w_gate,
    shift_mix,
    decay_base,
    rate_base,
    decay_drift,
    group_gain,
    initial_state,
    w_out,
):
    share, depth = tokens.shape
    width = w_recept.shape[1]
    seq = share * m
    span = share * m // 2
    heads, blocks = width // HEAD, seq // BLOCK
    hops = max(1, (n - 1).bit_length())
    lanes = 128
    vmem = pl.BlockSpec(memory_space=pltpu.VMEM)
    anywhere = pl.BlockSpec(memory_space=pl.ANY)
    dma = pltpu.SemaphoreType.DMA
    return pl.pallas_call(
        functools.partial(layer_kernel, n, m, heads, blocks),
        out_shape=jax.ShapeDtypeStruct((share, w_out.shape[1]), BF16),
        in_specs=[pl.BlockSpec(memory_space=pltpu.SMEM), anywhere, vmem]
        + [anywhere] * 6
        + [vmem] * 5
        + [anywhere],
        out_specs=vmem,
        scratch_shapes=[
            pltpu.VMEM((m, share, depth), BF16),
            pltpu.VMEM((depth // lanes, lanes), F32),
            pltpu.VMEM((2, depth // lanes, lanes), F32),
            pltpu.VMEM((span + 16, depth), BF16),
            pltpu.VMEM((6, depth, width), BF16),
            pltpu.VMEM((6, seq, width), BF16),
            pltpu.VMEM((3, 16, width), F32),
            pltpu.VMEM((3, 8, width), F32),
            pltpu.VMEM((blocks, heads, BLOCK, 2 * HEAD), F32),
            pltpu.VMEM((blocks, heads, BLOCK, 2 * HEAD), BF16),
            pltpu.VMEM((blocks, heads, 2 * BLOCK, 2 * HEAD), BF16),
            pltpu.VMEM((heads, seq, 2 * HEAD), F32),
            pltpu.VMEM((seq, width), F32),
            pltpu.VMEM((blocks, heads, HEAD, 2 * HEAD), F32),
            pltpu.VMEM((blocks, heads, HEAD, 2 * HEAD), F32),
            pltpu.VMEM((heads, HEAD, 2 * HEAD), F32),
            pltpu.VMEM((heads, HEAD, 2 * HEAD), F32),
            pltpu.VMEM((hops, heads, HEAD, 2 * HEAD), BF16),
            pltpu.VMEM((hops, heads, HEAD, 2 * HEAD), BF16),
            pltpu.VMEM((heads // 2, HEAD, 2 * HEAD), BF16),
            pltpu.VMEM((heads // 2, HEAD, 2 * HEAD), BF16),
            pltpu.VMEM((m - 1, share, width), BF16),
            pltpu.VMEM((m, share, width), BF16),
            pltpu.VMEM(w_out.shape, BF16),
            dma,
            dma((7,)),
            dma((m,)),
            dma((m,)),
            dma((chunks_of(share),)),
            dma((chunks_of(share),)),
            dma((m, chunks_of(share))),
            dma((m, chunks_of(share))),
            dma((m,)),
            dma((2,)),
            dma((hops,)),
            dma((hops,)),
            dma((m,)),
            dma((m,)),
        ],
        compiler_params=pltpu.CompilerParams(
            collective_id=1, has_side_effects=True, vmem_limit_bytes=60 * 1024 * 1024
        ),
        name="layer_kernel",
    )(
        decay_drift,
        tokens,
        norm_gain,
        w_recept,
        w_key,
        w_value,
        w_decay,
        w_rate,
        w_gate,
        shift_mix,
        decay_base,
        rate_base,
        group_gain,
        initial_state,
        w_out,
    )


def solution(mesh):
    return jax.shard_map(
        functools.partial(per_device, mesh.shape["sp"], mesh.shape["tp"]),
        mesh=mesh,
        in_specs=(
            P(("sp", "tp"), None),
            P(),
            P(None, "tp"),
            P(None, "tp"),
            P(None, "tp"),
            P(None, "tp"),
            P(None, "tp"),
            P(None, "tp"),
            P(None, "tp"),
            P("tp"),
            P("tp"),
            P("sp"),
            P("tp"),
            P("tp", None, None),
            P(),
        ),
        out_specs=P(("sp", "tp"), None),
        check_vma=False,
    )
```

```python
import functools

import jax
import jax.numpy as jnp
from jax import lax
from jax.experimental import pallas as pl
from jax.experimental.pallas import tpu as pltpu
from jax.sharding import PartitionSpec as P

HEAD = 64
BLOCK = 64
F32 = jnp.float32
BF16 = jnp.bfloat16

norm_floor = 0.5
group_floor = 1.0

NN = (((1,), (0,)), ((), ()))
NT = (((1,), (1,)), ((), ()))
TN = (((0,), (0,)), ((), ()))


def dot1(a, b, dims):
    return lax.dot_general(a, b, dims, preferred_element_type=F32)


def split(a):
    high = a.astype(BF16)
    return high, (a - high.astype(F32)).astype(BF16)


def mm(a, b, dims=NN):
    ah, al = split(a)
    bh, bl = split(b)
    return dot1(ah, bh, dims) + (dot1(ah, bl, dims) + dot1(al, bh, dims))


def mm1(a, b, dims=NN):
    return dot1(a.astype(BF16), b.astype(BF16), dims)


def mm2(a, b, dims=NN):
    ah, al = split(a)
    return dot1(ah, b, dims) + dot1(al, b, dims)


def sum_rows(a, ones):
    high, rest = split(a)
    mid, low = split(a - high.astype(F32))
    return dot1(ones, high, NN) + (dot1(ones, mid, NN) + dot1(ones, low, NN))


def chunks_of(share):
    return max(c for c in (1, 2, 3, 4) if share % (16 * c) == 0)


def layer_kernel(
    n,
    m,
    heads,
    blocks,
    drift_ref,
    tok_ref,
    ngain_ref,
    wr_ref,
    wk_ref,
    wv_ref,
    wd_ref,
    wa_ref,
    wg_ref,
    mix_ref,
    dbase_ref,
    rbase_ref,
    gain_ref,
    init_ref,
    out_ref,
    tok,
    edge_out,
    edge_in,
    normed,
    weights,
    proj,
    edges,
    last_row,
    reads,
    ups,
    stack,
    final_reads,
    gates,
    pieces,
    prefix,
    running,
    window,
    g_buf,
    r_buf,
    c_out,
    c_in,
    gated,
    act,
    own_sem,
    w_sem,
    t_send,
    t_recv,
    x_send,
    x_recv,
    f_send,
    f_recv,
    e_send,
    e_recv,
    g_send,
    g_recv,
    a_send,
    a_recv,
):
    s = lax.axis_index("sp")
    t = lax.axis_index("tp")
    half = m // 2
    upper = t // half
    base = upper * half
    across = lax.rem(t + half, m)
    share, depth = tok_ref.shape
    lanes = edge_out.shape[1]
    width = BLOCK
    channels = heads * HEAD
    steps = []
    while (1 << len(steps)) < n:
        steps.append(1 << len(steps))

    def near(q):
        return base + lax.rem(t - base + q, half)

    own_load = pltpu.make_async_copy(tok_ref, tok.at[t], own_sem)
    own_load.start()
    sources = (wr_ref, wk_ref, wv_ref, wd_ref, wa_ref, wg_ref)
    loads = [
        pltpu.make_async_copy(ref, weights.at[j], w_sem.at[j]) for j, ref in enumerate(sources)
    ]
    for load in loads:
        load.start()

    barrier = pltpu.get_barrier_semaphore()
    count = m - 1

    def greet(sp, tp):
        pl.semaphore_signal(
            barrier, inc=1, device_id={"sp": sp, "tp": tp}, device_id_type=pl.DeviceIdType.MESH
        )

    for q in range(1, m):
        greet(s, lax.rem(t + q, m))
    for d in steps:
        for other, ok in ((s + d, s + d < n), (s - d, s - d >= 0)):
            count = count + ok.astype(jnp.int32)

            @pl.when(ok)
            def _():
                greet(other, t)

    for q in range(m - 1):
        sends = jnp.logical_and(t == m - 1, s + 1 < n)
        takes = jnp.logical_and(t == q, s >= 1)
        count = count + sends.astype(jnp.int32) + takes.astype(jnp.int32)

        @pl.when(sends)
        def _():
            greet(s + 1, q)

        @pl.when(takes)
        def _():
            greet(s - 1, m - 1)

    own_load.wait()
    last = tok[t, share - 16 :, :].astype(F32)[15:16, :]
    for i in range(depth // lanes):
        edge_out[i : i + 1, :] = last[:, i * lanes : (i + 1) * lanes]
    pl.semaphore_wait(barrier, count)

    def remote(src, dst, send, recv, sp, tp):
        return pltpu.make_async_remote_copy(
            src_ref=src,
            dst_ref=dst,
            send_sem=send,
            recv_sem=recv,
            device_id={"sp": sp, "tp": tp},
            device_id_type=pl.DeviceIdType.MESH,
        )

    def token_copy(q):
        return remote(tok.at[t], tok.at[t], t_send.at[q], t_recv.at[q], s, near(q))

    chunks = chunks_of(share)
    rows_each = share // chunks

    def across_copy(c):
        some = tok.at[t, pl.ds(c * rows_each, rows_each), :]
        return remote(some, some, x_send.at[c], x_recv.at[c], s, across)

    def forward_copy(q, c):
        some = tok.at[across, pl.ds(c * rows_each, rows_each), :]
        return remote(some, some, f_send.at[q, c], f_recv.at[q, c], s, near(q))

    def edge_copy(q):
        return remote(edge_out, edge_in.at[0], e_send.at[q], e_recv.at[0], s + 1, q)

    def middle_copy(q):
        return remote(edge_out, edge_in.at[1], e_send.at[q], e_recv.at[1], s, half + q)

    has_next = jnp.logical_and(t == m - 1, s + 1 < n)
    has_middle = t == half - 1

    @pl.when(has_next)
    def _():
        for q in range(m):
            edge_copy(q).start()

    @pl.when(has_middle)
    def _():
        for q in range(half):
            middle_copy(q).start()

    for c in range(chunks):
        across_copy(c).start()
    for q in range(1, half):
        token_copy(q).start()

    rows_i = lax.broadcasted_iota(jnp.int32, (width, width), 0)
    cols_i = lax.broadcasted_iota(jnp.int32, (width, width), 1)
    strict = cols_i < rows_i
    incl = cols_i <= rows_i
    eye = jnp.where(cols_i == rows_i, 1.0, 0.0).astype(F32)
    ones = jnp.where(incl, 1.0, 0.0).astype(BF16)
    incl_two = jnp.concatenate([jnp.where(incl, 1.0, 0.0)] * 2, axis=1) > 0.5
    zeros = jnp.zeros((width, HEAD), F32)
    levels = []
    size = 1
    while size < width:
        same = (rows_i // (2 * size)) == (cols_i // (2 * size))
        levels.append(same & ((rows_i // size) % 2 == 1) & ((cols_i // size) % 2 == 0))
        size *= 2
    first_row = lax.broadcasted_iota(jnp.int32, (width, channels), 0) == 0
    mix = mix_ref[...]
    dbase = dbase_ref[...].reshape(1, channels)
    rbase = rbase_ref[...].reshape(1, channels)
    gain = gain_ref[...].reshape(1, channels)
    ngain = ngain_ref[...].reshape(1, depth)

    def norm(x):
        scale = lax.rsqrt(jnp.mean(x * x, axis=1, keepdims=True) + norm_floor)
        return (x * scale * ngain).astype(BF16)

    tile = 16
    span = half * share

    def norm_block(owner, place, begin=0, number=share):
        @pl.loop(0, number // tile)
        def _(i):
            rows = pl.ds(pl.multiple_of(begin + i * tile, tile), tile)
            to = pl.ds(pl.multiple_of(place * share + begin + i * tile, tile), tile)
            normed[to, :] = norm(tok[owner, rows, :].astype(F32))

    def project(first, extra):
        to = pl.ds(pl.multiple_of(first * share, share), span)
        for j in range(len(sources)):
            if extra:
                loads[j].wait()
            if extra and j < 3:
                made = dot1(normed[...], weights[j], NN).astype(BF16)
                edges[j] = made[span:, :].astype(F32)
                proj[j, to, :] = made[:span, :]
            else:
                proj[j, to, :] = dot1(normed[:span, :], weights[j], NN).astype(BF16)

    def prepare(bs):
        units, alphas, betas, keys, vals, fins, cross, recs = [], [], [], [], [], [], [], []
        for b in bs:
            at = pl.ds(pl.multiple_of(b * width, width), width)

            def shifted(j):
                cur = proj[j, at, :].astype(F32)
                earlier = jnp.where(first_row, last_row[j, 0:1, :], pltpu.roll(cur, 1, 0))
                last_row[j] = jnp.broadcast_to(cur[width - 1 :, :], (8, channels))
                return cur + (earlier - cur) * mix[j : j + 1, :]

            recept, key, value = shifted(0), shifted(1), shifted(2)
            level = dbase + proj[3, at, :].astype(F32) + drift_ref[b * width]
            logs = -0.6065306597126334 * jax.nn.sigmoid(level)
            rate = jax.nn.sigmoid(rbase + proj[4, at, :].astype(F32))
            total = sum_rows(logs, ones)
            through = jnp.exp(total)
            until = jnp.exp(total - logs)
            inverse = jnp.exp(-total)
            key_s = key * inverse
            rec_s = recept * through
            final = through[width - 1 :, :]
            rate_inv = rate * inverse
            for h in range(heads):
                ch = slice(h * HEAD, (h + 1) * HEAD)
                key_h = key[:, ch]
                unit = key_h * lax.rsqrt(jnp.sum(key_h * key_h, axis=1, keepdims=True) + 1.0)
                units.append((b, h))
                alphas.append(-unit * until[:, ch])
                betas.append(unit * rate_inv[:, ch])
                keys.append(key_s[:, ch])
                vals.append(value[:, ch])
                fins.append(final[:, ch])
                recs.append(rec_s[:, ch])
                reads[b, h, :, :HEAD] = rec_s[:, ch]
        every = range(len(units))
        cross = [
            mm(
                jnp.concatenate([alphas[u], recs[u]], axis=0),
                jnp.concatenate([betas[u], keys[u]], axis=0),
                NT,
            )
            for u in every
        ]
        for u in every:
            ups[units[u]] = jnp.where(incl_two, cross[u][width:, :], 0.0).astype(BF16)
        low_ab = [jnp.where(strict, c[:width, :width], 0.0) for c in cross]
        low_ak = [jnp.where(strict, c[:width, width:], 0.0) for c in cross]
        both = [mm(low_ak[u], vals[u]) for u in every]
        inv = [eye + jnp.where(levels[0], low, 0.0) for low in low_ab]
        for mask in levels[1:]:
            short = [i.astype(BF16) for i in inv]
            right = [mm1(jnp.where(mask, low_ab[u], 0.0), short[u]) for u in every]
            inv = [inv[u] + mm1(short[u], right[u]) for u in every]
        solved = [mm(inv[u], jnp.concatenate([alphas[u], both[u]], axis=1)) for u in every]
        for u in every:
            ends = jnp.concatenate([betas[u] * fins[u], keys[u] * fins[u]], axis=0)
            column = jnp.concatenate(
                [solved[u], jnp.concatenate([zeros, vals[u]], axis=1)], axis=0
            )
            stack[units[u]] = column.astype(BF16)
            pieces[units[u]] = mm(ends, column, TN) + jnp.concatenate(
                [eye * fins[u], zeros], axis=1
            )

    def centered(x):
        return x - jnp.mean(x, axis=1, keepdims=True)

    def defer(b):
        at = pl.ds(pl.multiple_of(b * width, width), width)
        for h in range(heads):
            made = dot1(ups[b, h], stack[b, h], NN)
            read = reads[b, h, :, :HEAD] + made[:, :HEAD]
            both = mm(read, prefix[b, h])
            fixed = centered(both[:, HEAD:] + made[:, HEAD:])
            final_reads[h, at, :] = jnp.concatenate([both[:, :HEAD], fixed], axis=1)
        gates[at, :] = jax.nn.sigmoid(proj[5, at, :].astype(F32)) * gain

    def open_half(which):
        for j in range(3):
            row = jnp.where(which == 0, edges[j, 0:1, :], edges[j, 1:2, :])
            last_row[j] = jnp.broadcast_to(row, (8, channels))

    norm_block(t, t - base)
    for q in range(1, half):
        token_copy(q).wait_recv()
        norm_block(near(half - q), near(half - q) - base)

    @pl.when(s >= 1)
    def _():
        remote(edge_out, edge_in.at[0], e_send.at[0], e_recv.at[0], s, t).wait_recv()

    @pl.when(s == 0)
    def _():
        edge_in[0] = jnp.zeros(edge_in.shape[1:], F32)

    @pl.when(upper == 1)
    def _():
        remote(edge_out, edge_in.at[1], e_send.at[0], e_recv.at[1], s, t).wait_recv()

    @pl.when(upper == 0)
    def _():
        row = tok[half - 1, share - 16 :, :].astype(F32)[15:16, :]
        for i in range(depth // lanes):
            edge_in[1, i : i + 1, :] = row[:, i * lanes : (i + 1) * lanes]

    joined_rows = [
        jnp.concatenate([edge_in[k, i : i + 1, :] for i in range(depth // lanes)], axis=1)
        for k in range(2)
    ]
    normed[span:, :] = norm(
        jnp.concatenate(joined_rows + [jnp.zeros((14, depth), F32)], axis=0)
    )
    project(base, True)
    open_half(upper)

    group = max(g for g in (1, 2, 3) if (blocks // 2) % g == 0)

    def prepare_half(first):
        @pl.loop(0, blocks // 2 // group)
        def _(i):
            prepare([first + i * group + g for g in range(group)])

    prepare_half(upper * (blocks // 2))

    lower = 1 - upper
    for c in range(chunks):
        across_copy(c).wait_recv()
        for q in range(1, half):
            forward_copy(q, c).start()
        norm_block(across, across - lower * half, c * rows_each, rows_each)
    for q in range(1, half):
        far = lower * half + near(half - q) - base
        for c in range(chunks):
            forward_copy(q, c).wait_recv()
            norm_block(far, far - lower * half, c * rows_each, rows_each)
    project(lower * half, False)
    open_half(lower)

    prepare_half(lower * (blocks // 2))

    def joined(later, earlier):
        return mm(later[:, :HEAD], earlier) + jnp.concatenate([zeros, later[:, HEAD:]], axis=1)

    for h in range(heads):
        running[h] = jnp.concatenate([eye, zeros], axis=1)

    @pl.loop(0, blocks)
    def _(b):
        for h in range(heads):
            prefix[b, h] = running[h]
            running[h] = joined(pieces[b, h], running[h])

    at_start = s == 0
    for h in range(heads):
        own = running[h]
        start = jnp.concatenate([zeros, init_ref[h].T], axis=1)
        window[h] = jnp.where(at_start, start, jnp.concatenate([eye, zeros], axis=1))
        whole = jnp.where(at_start, joined(own, start), own)
        running[h] = whole

    final_hop = len(steps) - 1

    def offer(k, wholes):
        if k < final_hop:
            for h in range(heads):
                g_buf[k, h] = wholes[h].astype(BF16)
        else:
            for p in range(heads // 2):
                pair = [wholes[2 * p][:, HEAD:], wholes[2 * p + 1][:, HEAD:]]
                c_out[p] = jnp.concatenate(pair, axis=1).astype(BF16)

    offer(0, [running[h] for h in range(heads)])

    def hop(k):
        src, dst = (g_buf.at[k], r_buf.at[k]) if k < final_hop else (c_out, c_in)
        return remote(src, dst, g_send.at[k], g_recv.at[k], s + steps[k], t)

    for k, d in enumerate(steps):

        @pl.when(s + d < n)
        def _():
            hop(k).start()

        @pl.loop(k * blocks // len(steps), (k + 1) * blocks // len(steps))
        def _(b):
            defer(b)

        @pl.when(s - d >= 0)
        def _():
            hop(k).wait_recv()
            for h in range(heads):
                now = window[h]
                if k < final_hop:
                    window[h] = mm2(now[:, :HEAD], r_buf[k, h]) + jnp.concatenate(
                        [zeros, now[:, HEAD:]], axis=1
                    )
                else:
                    lane = (h % 2) * HEAD
                    got = mm2(now[:, :HEAD], c_in[h // 2])[:, lane : lane + HEAD]
                    window[h] = jnp.concatenate([zeros, got + now[:, HEAD:]], axis=1)

        if k + 1 < len(steps):
            offer(
                k + 1,
                [
                    jnp.where(at_start, running[h], joined(running[h], window[h]))
                    for h in range(heads)
                ],
            )

    entry = [split(centered(window[h][:, HEAD:])) for h in range(heads)]

    def finish(dest):
        at = pl.ds(pl.multiple_of(dest * share, share), share)
        parts = []
        for h in range(heads):
            read = final_reads[h, at, :]
            high, low = split(read[:, :HEAD])
            center = dot1(high, entry[h][0], NN) + (
                dot1(high, entry[h][1], NN) + dot1(low, entry[h][0], NN)
            )
            center = center + read[:, HEAD:]
            spread = jnp.mean(center * center, axis=1, keepdims=True)
            parts.append(center * lax.rsqrt(spread + group_floor))
        return (jnp.concatenate(parts, axis=1) * gates[at, :]).astype(BF16)

    def part(q):
        dest = lax.rem(t + q, m)
        return remote(gated.at[q - 1], act.at[t], a_send.at[q], a_recv.at[q], s, dest)

    for q in range(1, m):
        gated[q - 1] = finish(lax.rem(t + q, m))
        part(q).start()
    act[t] = finish(t)
    for q in range(1, m):
        part(q).wait_recv()
    for q in range(m):
        out_ref[:, q * channels : (q + 1) * channels] = act[q]
    for q in range(1, m):
        part(q).wait_send()
    for c in range(chunks):
        across_copy(c).wait_send()
    for q in range(1, half):
        token_copy(q).wait_send()
        for c in range(chunks):
            forward_copy(q, c).wait_send()

    @pl.when(has_next)
    def _():
        for q in range(m):
            edge_copy(q).wait_send()

    @pl.when(has_middle)
    def _():
        for q in range(half):
            middle_copy(q).wait_send()

    for k, d in enumerate(steps):

        @pl.when(s + d < n)
        def _():
            hop(k).wait_send()


def per_device(
    n,
    m,
    tokens,
    norm_gain,
    w_recept,
    w_key,
    w_value,
    w_decay,
    w_rate,
    w_gate,
    shift_mix,
    decay_base,
    rate_base,
    decay_drift,
    group_gain,
    initial_state,
    w_out,
):
    share, depth = tokens.shape
    width = w_recept.shape[1]
    seq = share * m
    span = share * m // 2
    heads, blocks = width // HEAD, seq // BLOCK
    hops = max(1, (n - 1).bit_length())
    lanes = 128
    vmem = pl.BlockSpec(memory_space=pltpu.VMEM)
    anywhere = pl.BlockSpec(memory_space=pltpu.MemorySpace.HBM)
    dma = pltpu.SemaphoreType.DMA
    rows = pl.pallas_call(
        functools.partial(layer_kernel, n, m, heads, blocks),
        out_shape=jax.ShapeDtypeStruct((share, m * width), BF16),
        in_specs=[pl.BlockSpec(memory_space=pltpu.SMEM), anywhere, vmem]
        + [anywhere] * 6
        + [vmem] * 5,
        out_specs=vmem,
        scratch_shapes=[
            pltpu.VMEM((m, share, depth), BF16),
            pltpu.VMEM((depth // lanes, lanes), F32),
            pltpu.VMEM((2, depth // lanes, lanes), F32),
            pltpu.VMEM((span + 16, depth), BF16),
            pltpu.VMEM((6, depth, width), BF16),
            pltpu.VMEM((6, seq, width), BF16),
            pltpu.VMEM((3, 16, width), F32),
            pltpu.VMEM((3, 8, width), F32),
            pltpu.VMEM((blocks, heads, BLOCK, 2 * HEAD), F32),
            pltpu.VMEM((blocks, heads, BLOCK, 2 * HEAD), BF16),
            pltpu.VMEM((blocks, heads, 2 * BLOCK, 2 * HEAD), BF16),
            pltpu.VMEM((heads, seq, 2 * HEAD), F32),
            pltpu.VMEM((seq, width), F32),
            pltpu.VMEM((blocks, heads, HEAD, 2 * HEAD), F32),
            pltpu.VMEM((blocks, heads, HEAD, 2 * HEAD), F32),
            pltpu.VMEM((heads, HEAD, 2 * HEAD), F32),
            pltpu.VMEM((heads, HEAD, 2 * HEAD), F32),
            pltpu.VMEM((hops, heads, HEAD, 2 * HEAD), BF16),
            pltpu.VMEM((hops, heads, HEAD, 2 * HEAD), BF16),
            pltpu.VMEM((heads // 2, HEAD, 2 * HEAD), BF16),
            pltpu.VMEM((heads // 2, HEAD, 2 * HEAD), BF16),
            pltpu.VMEM((m - 1, share, width), BF16),
            pltpu.VMEM((m, share, width), BF16),
            dma,
            dma((6,)),
            dma((m,)),
            dma((m,)),
            dma((chunks_of(share),)),
            dma((chunks_of(share),)),
            dma((m, chunks_of(share))),
            dma((m, chunks_of(share))),
            dma((m,)),
            dma((2,)),
            dma((hops,)),
            dma((hops,)),
            dma((m,)),
            dma((m,)),
        ],
        compiler_params=pltpu.CompilerParams(
            collective_id=1, has_side_effects=True, vmem_limit_bytes=40 * 1024 * 1024
        ),
        name="layer_kernel",
    )(
        decay_drift,
        tokens,
        norm_gain,
        w_recept,
        w_key,
        w_value,
        w_decay,
        w_rate,
        w_gate,
        shift_mix,
        decay_base,
        rate_base,
        group_gain,
        initial_state,
    )
    return jnp.dot(rows, w_out, preferred_element_type=F32).astype(BF16)


def solution(mesh):
    return jax.shard_map(
        functools.partial(per_device, mesh.shape["sp"], mesh.shape["tp"]),
        mesh=mesh,
        in_specs=(
            P(("sp", "tp"), None),
            P(),
            P(None, "tp"),
            P(None, "tp"),
            P(None, "tp"),
            P(None, "tp"),
            P(None, "tp"),
            P(None, "tp"),
            P(None, "tp"),
            P("tp"),
            P("tp"),
            P("sp"),
            P("tp"),
            P("tp", None, None),
            P(),
        ),
        out_specs=P(("sp", "tp"), None),
        check_vma=False,
    )
```
